512 devices in a mesh: ep: 128 (over z, y, core), tp: 4 (over x).
Axes of the slice: x: 4, y: 8, z: 8, core: 2. Of those that a mesh axis runs over, the one named last changes fastest.
Arguments:
- tokens: bfloat16 [16384, 2048], P('ep'), may hold values from -6 to 6
- cotangent: bfloat16 [16384, 2048], P('ep'), may hold values from -6 to 6
- route_weights: float32 [16384, 2], P('ep'), may hold values from 0.25 to 2.5
- routes: int32 [16384, 2], P('ep'), may hold values from 0 to 127, all different within a row; in each aligned block of 128 rows (0 to 127, 128 to 255, ...) at most 4 rows name the same one
- gate_proj: bfloat16 [128, 2048, 512], P('ep', None, 'tp'), may hold values from -0.125 to 0.125
- up_proj: bfloat16 [128, 2048, 512], P('ep', None, 'tp'), may hold values from -0.125 to 0.125
- down_proj: bfloat16 [128, 512, 2048], P('ep', 'tp'), may hold values from -0.25 to 0.25
- shared_down: bfloat16 [2048, 512], P(None, 'tp'), may hold values from -0.25 to 0.25
- shared_hidden: bfloat16 [16384, 512], P('ep', 'tp'), may hold values from -0.29882812 to 0.29882812
Outputs:
- tokens_grad: bfloat16 [16384, 2048], P('ep', 'tp')
- weights_grad: float32 [16384, 2], P('ep')
- gate_proj_grad: bfloat16 [128, 2048, 512], P('ep', None, 'tp')
- up_proj_grad: bfloat16 [128, 2048, 512], P('ep', None, 'tp')
- down_proj_grad: bfloat16 [128, 512, 2048], P('ep', 'tp')
- hidden_grad: bfloat16 [16384, 512], P('ep', 'tp')
- shared_grad: float32 [2048, 512], P('ep', 'tp')
The draws below stay inside these ranges and needn't reach their ends.
Inputs may be any that keep to these rules, and one draw needn't show every extreme that they name: `routes`: in each aligned block of 128 rows no expert is named more than 4 times, a bound that some block reaches; the 2 experts of a row differ.
All inputs are finite; a program needn't handle non-finite values.
Results may differ from the reference program's by a relative error of at most 0.012.
Values may be sent and summed in bfloat16 or wider, within the bound.
No kernel may reach another device: no remote copies, remote signals or barrier semaphores. Data moves between devices by JAX's collectives and lax.ppermute only.
A program may use at most 64 MiB of HBM per device.

```python
import math
import jax
import jax.numpy as jnp
import numpy as np
from jax import lax

D = 2048
FF = 512
D_SHARED = 512
TOP = 2
TOK_DEV = 128
EXPERTS = 128
TOKENS = 16384
CAP = 4
N_EP = 128
N_TP = 4


def raised(values, stream_key, source, target, parts, factor):
    def block_of(position):
        return (jnp.arange(values.shape[position]) // (values.shape[position] // parts)).reshape((-1,) + (1,) * (values.ndim - 1 - position))

    near = jax.random.permutation(stream_key, parts)[block_of(target)]
    other_side = (block_of(target) + parts // 2) % parts
    return jnp.where((block_of(source) == near) | (block_of(source) == other_side), factor * values, values)


def block_levels(stream_key, extent, shards, low, top_value):
    factor_of, own = 1.0, jax.random.fold_in(stream_key, 6)
    for axis_at, shards_of in shards:
        draws = jnp.exp(jax.random.uniform(jax.random.fold_in(own, axis_at), (shards_of,), jnp.float32, low / len(shards), top_value / len(shards)))
        factor_of = factor_of * jnp.repeat(draws, extent[axis_at] // shards_of).reshape([-1 if axis == axis_at else 1 for axis in range(len(extent))])
    return factor_of


def assign_block(rng, own, number, rows, count, top, limit, lean):
    sequence = jax.random.permutation(rng, count)
    heavy_load, common = load_shares(count, rows * top, limit, lean, True), load_shares(count, rows * top, limit, lean, False)
    places = jnp.arange(count)

    def named(sizes, turn):
        used = int((sizes > 0).sum())
        fixed = max(1, used // 4)
        passed = fixed + (places - fixed + turn * (used - fixed)) % max(1, count - fixed)
        return jnp.zeros((count,), jnp.int32).at[sequence[jnp.where(places < fixed, places, passed)]].set(jnp.asarray(sizes, jnp.int32))

    sizes = jnp.where(number % 4 == 0, named(heavy_load, number // 4), named(common, number - number // 4 - 1))
    mixed = jax.random.permutation(jax.random.fold_in(own, 3), count)
    donor, sink = mixed[0:count // 2 * 2:2], mixed[1:count // 2 * 2:2]
    margin = jnp.minimum(sizes[donor] - 1, limit - sizes[sink]) // 2
    margin = jnp.where((donor == sequence[0]) | (sink == sequence[0]) | (sizes[sink] == 0), 0, jnp.maximum(margin, 0))
    passed = jax.random.randint(jax.random.fold_in(own, 4), (count // 2,), 0, 1 << 20) % (margin + 1)
    sizes = sizes.at[donor].add(-passed).at[sink].add(passed)
    items = jnp.searchsorted(jnp.cumsum(sizes), jnp.arange(rows * top), side="right").astype(jnp.int32)
    grid = items.reshape(top, rows).T
    grid = grid[jax.random.permutation(jax.random.fold_in(own, 1), rows)]
    turn = jax.random.randint(jax.random.fold_in(own, 2), (rows, 1), 0, top)
    return jnp.take_along_axis(grid, (jnp.arange(top)[None, :] + turn) % top, axis=1)


def load_shares(number_of, total, limit, lean, full):
    loads = [(1 << 20) // math.isqrt(rank ** lean) + 1 for rank in range(1, number_of + 1)]
    largest = limit if full else min(limit, max(-(-total // number_of), total * loads[0] // sum(loads)))
    least = 1 if total - largest >= number_of - 1 else 0
    counts, spare = [largest] + [least] * (number_of - 1), total - largest - least * (number_of - 1)
    while spare > 0:
        free = [i for i in range(1, number_of) if counts[i] < largest] or [i for i in range(1, number_of) if counts[i] < limit]
        mass, budget = sum([loads[i] for i in free]), spare
        for i in free:
            extra = min(limit - counts[i], max(1, budget * loads[i] // mass), spare)
            counts[i] = counts[i] + extra
            spare = spare - extra
    return np.array(counts)


def centred(own_key, shape, spread, limit, shards=(), kind=jnp.bfloat16):
    result = spread * jax.random.normal(own_key, shape, jnp.float32)
    if shards:
        result = result * block_levels(own_key, shape, shards, -0.22, 0.18)
    return jnp.clip(result, -limit, limit).astype(kind)


def noise_with(rng, extent, scale, most, split, heavy, kind=jnp.bfloat16):
    drawn = scale * jax.random.normal(rng, extent, jnp.float32)
    if split:
        drawn = drawn * block_levels(rng, extent, split, -0.22, 0.18)
    return jnp.clip(raised(drawn, jax.random.fold_in(rng, 3), *heavy), -most, most).astype(kind)


def setup_inputs(seed: int = 0) -> dict:
    seeds = jax.random.split(jax.random.key(seed), 10)
    tokens = centred(seeds[0], (TOKENS, D), 1.0, 6.0, ((0, 128),))
    cotangent = noise_with(seeds[1], (TOKENS, D), 0.25, 6.0, ((0, 128),), (0, 1, 128, 5.5))
    route_weights = jnp.clip(jnp.exp(math.log(2.5) - 2.3025851 * jax.random.uniform(seeds[2], (TOKENS, TOP), jnp.float32) ** block_levels(seeds[2], (TOKENS, TOP), ((0, 128),), -0.2, 0.2)), 0.25, 2.5)
    routes_keys = jax.random.split(jax.random.fold_in(seeds[3], 1), TOKENS // TOK_DEV)
    routes_turns = jax.random.permutation(jax.random.fold_in(seeds[3], 3), TOKENS // TOK_DEV)
    routes = jax.vmap(lambda own, number: assign_block(jax.random.fold_in(seeds[3], 2), own, number, TOK_DEV, EXPERTS, TOP, CAP, 2))(routes_keys, routes_turns).reshape((TOKENS, TOP))
    gate_proj = centred(seeds[4], (EXPERTS, D, FF), D ** -0.5, 0.125, ((0, 128), (2, 4)))
    up_proj = centred(seeds[5], (EXPERTS, D, FF), D ** -0.5, 0.125, ((0, 128), (2, 4)))
    down_proj = centred(seeds[6], (EXPERTS, FF, D), FF ** -0.5, 0.25, ((0, 128), (1, 4)))
    shared_down = centred(seeds[7], (D, D_SHARED), D_SHARED ** -0.5, 0.25, ((1, 4),))
    shared_hidden = centred(seeds[8], (TOKENS, D_SHARED), 0.05, 0.29882812, ((0, 128), (1, 4)))
    return {"tokens": tokens, "cotangent": cotangent, "route_weights": route_weights, "routes": routes, "gate_proj": gate_proj, "up_proj": up_proj, "down_proj": down_proj, "shared_down": shared_down, "shared_hidden": shared_hidden}


def slot_index(routes):
    blocks = routes.reshape(N_EP, TOK_DEV * TOP)
    one_hot = (blocks[:, :, None] == jnp.arange(EXPERTS, dtype=jnp.int32)[None, None, :]).astype(jnp.int32)
    earlier = jnp.cumsum(one_hot, axis=1) - one_hot
    rank_in = jnp.sum(earlier * one_hot, axis=2)
    source = jnp.arange(N_EP, dtype=jnp.int32)[:, None]
    return ((blocks * N_EP + source) * CAP + rank_in).astype(jnp.int32)


def one_expert(inputs):
    in_rows, in_grads, in_weights, w_gate, w_up, w_down = inputs
    gate = jnp.dot(in_rows, w_gate, preferred_element_type=jnp.float32)
    upper = jnp.dot(in_rows, w_up, preferred_element_type=jnp.float32)
    active = jax.nn.silu(gate)
    hidden = (active * upper).astype(jnp.bfloat16)
    backed = jnp.dot(in_grads, w_down.T, preferred_element_type=jnp.float32)
    gate_grad = jnp.sum(hidden.astype(jnp.float32) * backed, axis=1).astype(jnp.bfloat16)
    weight_col = in_weights.astype(jnp.float32)[:, None]
    d_hidden = weight_col * backed
    sigma = jax.nn.sigmoid(gate)
    d_gate = (d_hidden * upper * sigma * (1.0 + gate * (1.0 - sigma))).astype(jnp.bfloat16)
    d_up = (d_hidden * active).astype(jnp.bfloat16)
    scaled = (weight_col * in_grads.astype(jnp.float32)).astype(jnp.bfloat16)
    down_grad = jnp.dot(hidden.T, scaled, preferred_element_type=jnp.float32).astype(jnp.bfloat16)
    gate_wgrad = jnp.dot(in_rows.T, d_gate, preferred_element_type=jnp.float32).astype(jnp.bfloat16)
    up_wgrad = jnp.dot(in_rows.T, d_up, preferred_element_type=jnp.float32).astype(jnp.bfloat16)
    block_units = FF // N_TP
    slot_count = in_rows.shape[0]
    dg_blocks = d_gate.astype(jnp.float32).reshape(slot_count, N_TP, block_units)
    du_blocks = d_up.astype(jnp.float32).reshape(slot_count, N_TP, block_units)
    wg_blocks = w_gate.astype(jnp.float32).reshape(D, N_TP, block_units)
    wu_blocks = w_up.astype(jnp.float32).reshape(D, N_TP, block_units)
    partial_value = jnp.einsum("rtf,dtf->trd", dg_blocks, wg_blocks) + jnp.einsum("rtf,dtf->trd", du_blocks, wu_blocks)
    partial_value = lax.optimization_barrier(partial_value.astype(jnp.bfloat16))
    input_grad = jnp.sum(partial_value.astype(jnp.float32), axis=0).astype(jnp.bfloat16)
    return input_grad, gate_grad, gate_wgrad, up_wgrad, down_grad


def reference(tokens, cotangent, route_weights, routes, gate_proj, up_proj, down_proj, shared_down, shared_hidden):
    slot_ids = slot_index(routes).reshape(-1)
    owner_ids = jnp.arange(TOKENS * TOP, dtype=jnp.int32) // TOP
    total_slots = EXPERTS * N_EP * CAP
    per_expert = N_EP * CAP
    row_buf = jnp.zeros((total_slots, D), jnp.bfloat16).at[slot_ids].set(tokens[owner_ids])
    grad_buf = jnp.zeros((total_slots, D), jnp.bfloat16).at[slot_ids].set(cotangent[owner_ids])
    weight_buf = jnp.zeros((total_slots,), jnp.bfloat16).at[slot_ids].set(route_weights.reshape(-1).astype(jnp.bfloat16))
    results = lax.map(one_expert, (row_buf.reshape(EXPERTS, per_expert, D), grad_buf.reshape(EXPERTS, per_expert, D),
                                   weight_buf.reshape(EXPERTS, per_expert), gate_proj, up_proj, down_proj))
    input_grad, gate_grad, gate_wgrad, up_wgrad, down_grad = results
    picked = input_grad.reshape(total_slots, D)[slot_ids].reshape(TOKENS, TOP, D)
    tokens_grad = jnp.sum(picked.astype(jnp.float32), axis=1).astype(jnp.bfloat16)
    weights_grad = gate_grad.reshape(total_slots)[slot_ids].astype(jnp.float32).reshape(TOKENS, TOP)
    hidden_grad = jnp.dot(cotangent, shared_down, preferred_element_type=jnp.float32).astype(jnp.bfloat16)
    shared_grad = jnp.dot(cotangent.T, shared_hidden, preferred_element_type=jnp.float32)
    return tokens_grad, weights_grad, gate_wgrad, up_wgrad, down_grad, hidden_grad, shared_grad
```

```python
import functools

import jax
import jax.numpy as jnp
from jax import lax
from jax.experimental import pallas as pl
from jax.experimental.pallas import tpu as pltpu
from jax.sharding import PartitionSpec as P

F32 = jnp.float32
BF16 = jnp.bfloat16
ROWS = (((0,), (0,)), ((), ()))
LAST = (((1,), (1,)), ((), ()))
VMEM = pl.BlockSpec(memory_space=pltpu.VMEM)
SMEM = pl.BlockSpec(memory_space=pltpu.SMEM)


def exchange(array, axis):
    return lax.all_to_all(array, axis, split_axis=0, concat_axis=0, tiled=True)


def mm(a, b, dims=(((1,), (0,)), ((), ()))):
    return lax.dot_general(a, b, dims, preferred_element_type=F32)


def chosen(routes_ref, slots, capacity):
    count = routes_ref.shape[1]
    row = lax.broadcasted_iota(jnp.int32, (slots, count), 0)
    expert = row // capacity
    first = expert == routes_ref[0:1, :]
    second = expert == routes_ref[1:2, :]
    named = jnp.where(first | second, 1.0, 0.0)
    earlier = lax.broadcasted_iota(jnp.int32, (count, count), 0)
    later = lax.broadcasted_iota(jnp.int32, (count, count), 1)
    before = jnp.where(earlier < later, 1.0, 0.0).astype(BF16)
    rank = mm(named.astype(BF16), before)
    place = (row - expert * capacity).astype(F32)
    hit = jnp.where(rank == place, named, 0.0)
    return hit, jnp.where(first, hit, 0.0), jnp.where(second, hit, 0.0)


def dispatch_kernel(col, routes_ref, weights_ref, tok_ref, cot_ref, x_ref, g_ref, pick_ref, *, cap):
    slots = x_ref.shape[0]
    hit, one, two = chosen(routes_ref, slots, cap)
    weights = weights_ref[...].astype(BF16).astype(F32)
    weight = jnp.sum(one * weights[0:1, :] + two * weights[1:2, :], axis=1, keepdims=True)
    pick = hit.astype(BF16)
    pick_ref[...] = pick
    x_ref[...] = mm(pick, tok_ref[...]).astype(BF16)
    g_ref[...] = (weight * mm(pick, cot_ref[...])).astype(BF16)


def dispatch(col, routes, weights, tokens, cotangent, slots, cap, quarter):
    rows = tokens.shape[0]
    whole = lambda *shape: pl.BlockSpec(shape, lambda i, col: (0,) * len(shape))
    part = pl.BlockSpec((rows, quarter), lambda i, col: (0, col[0]))
    return pl.pallas_call(
        functools.partial(dispatch_kernel, cap=cap),
        grid_spec=pltpu.PrefetchScalarGridSpec(
            num_scalar_prefetch=1,
            grid=(1,),
            in_specs=[whole(*routes.shape), whole(*weights.shape), part, part],
            out_specs=[whole(slots, quarter), whole(slots, quarter), whole(slots, rows)],
        ),
        out_shape=[
            jax.ShapeDtypeStruct((slots, quarter), BF16),
            jax.ShapeDtypeStruct((slots, quarter), BF16),
            jax.ShapeDtypeStruct((slots, rows), BF16),
        ],
        name="dispatch",
    )(col, routes, weights, tokens, cotangent)


def beside(ref):
    return jnp.concatenate([ref[k] for k in range(ref.shape[0])], axis=1)


def stacked(ref):
    return ref[...].reshape(-1, ref.shape[-1])


def local(kernel, out, name, *args, smem=0):
    return pl.pallas_call(
        kernel,
        in_specs=[SMEM] * smem + [VMEM] * (len(args) - smem),
        out_specs=jax.tree.map(lambda _: VMEM, out),
        out_shape=out,
        name=name,
    )(*args)


def partial_kernel(x_ref, g_ref, gate_ref, up_ref, down_ref, y_ref):
    hidden = y_ref.shape[1] // 3
    x = x_ref[...]
    y_ref[:, :hidden] = mm(x, beside(gate_ref)).astype(BF16)
    y_ref[:, hidden : 2 * hidden] = mm(x, beside(up_ref)).astype(BF16)
    y_ref[:, 2 * hidden :] = mm(g_ref[...], stacked(down_ref), LAST).astype(BF16)


def middle_kernel(col, y_ref, grads_ref, hidden_ref, share_ref):
    parts, rows, width = y_ref.shape
    hidden = width // 3
    total = y_ref[0].astype(F32)
    for k in range(1, parts):
        total = total + y_ref[k].astype(F32)
    gate = total[:, :hidden]
    upper = total[:, hidden : 2 * hidden]
    backed = total[:, 2 * hidden :]
    sigma = jax.nn.sigmoid(gate)
    active = gate * sigma
    hid = (active * upper).astype(BF16)
    d_gate = (backed * upper * sigma * (1.0 + gate * (1.0 - sigma))).astype(BF16)
    d_up = (backed * active).astype(BF16)
    share = jnp.sum(hid.astype(F32) * backed, axis=1, keepdims=True)
    share = jnp.broadcast_to(share, (rows, share_ref.shape[1]))
    for k in range(parts):
        grads_ref[k, :, :hidden] = d_gate
        grads_ref[k, :, hidden:] = d_up
        hidden_ref[k] = hid
        share_ref[k * rows : (k + 1) * rows, :] = jnp.where(col[0] == k, share, 0.0).astype(BF16)


def input_kernel(grads_ref, gate_ref, up_ref, out_ref):
    hidden = grads_ref.shape[2] // 2
    grads = stacked(grads_ref)
    out = mm(grads[:, :hidden], beside(gate_ref), LAST)
    out = out + mm(grads[:, hidden:], beside(up_ref), LAST)
    out_ref[...] = out.astype(BF16)


def weight_kernel(x_ref, grads_ref, gate_ref, up_ref):
    parts, _, block = gate_ref.shape
    hidden = grads_ref.shape[2] // 2
    grads = stacked(grads_ref)
    out = mm(x_ref[...], grads, ROWS).astype(BF16)
    for k in range(parts):
        gate_ref[k] = out[:, k * block : (k + 1) * block]
        up_ref[k] = out[:, hidden + k * block : hidden + (k + 1) * block]


def down_kernel(hidden_ref, g_ref, out_ref):
    out = mm(stacked(hidden_ref), g_ref[...], ROWS).astype(BF16)
    out_ref[...] = out.reshape(out_ref.shape)


def share_kernel(routes_ref, weights_ref, share_ref, out_ref, *, cap):
    _, one, two = chosen(routes_ref, share_ref.shape[0], cap)
    share = share_ref[...].astype(F32)
    weights = weights_ref[...].astype(BF16).astype(F32)
    out_ref[0:1, :] = jnp.sum(one * share, axis=0, keepdims=True) / weights[0:1, :]
    out_ref[1:2, :] = jnp.sum(two * share, axis=0, keepdims=True) / weights[1:2, :]


def combine_kernel(pick_ref, back_ref, out_ref):
    out_ref[...] = mm(pick_ref[...], back_ref[...], ROWS).astype(BF16)


def shards(
    tokens,
    cotangent,
    route_weights,
    routes,
    gate_proj,
    up_proj,
    down_proj,
    shared_down,
    shared_hidden,
):
    shape = jax.ShapeDtypeStruct
    rows, feat = tokens.shape
    top = routes.shape[1]
    ep = lax.axis_size("ep")
    tp = lax.axis_size("tp")
    experts = gate_proj.shape[0] * ep
    cap = 2 * rows * top // experts
    slots = experts * cap
    quarter = feat // tp
    block = gate_proj.shape[2]
    hidden = block * tp
    col = lax.axis_index("tp").astype(jnp.int32).reshape(1)
    routes_t = routes.T
    weights_t = route_weights.T

    w_gate = exchange(gate_proj.reshape(tp, quarter, block), "tp")
    w_up = exchange(up_proj.reshape(tp, quarter, block), "tp")
    w_down = exchange(
        down_proj.reshape(block, tp, quarter).transpose(1, 0, 2), "tp"
    )

    x, g, pick = dispatch(col, routes_t, weights_t, tokens, cotangent, slots, cap, quarter)
    x = exchange(x.reshape(ep, -1, quarter), "ep").reshape(slots, quarter)
    g = exchange(g.reshape(ep, -1, quarter), "ep").reshape(slots, quarter)

    part = local(partial_kernel, shape((slots, 3 * hidden), BF16), "partial", x, g, w_gate, w_up, w_down)
    part = exchange(part.reshape(tp, slots // tp, 3 * hidden), "tp")
    grads, hid, share = local(
        middle_kernel,
        (
            shape((tp, slots // tp, 2 * hidden), BF16),
            shape((tp, slots // tp, hidden), BF16),
            shape((slots, rows), BF16),
        ),
        "middle",
        col,
        part,
        smem=1,
    )
    grads = exchange(grads, "tp")
    hid = exchange(hid, "tp")
    share = exchange(share.reshape(ep, -1, rows), "ep").reshape(slots, rows)

    back = local(input_kernel, shape((slots, quarter), BF16), "input", grads, w_gate, w_up)
    back = exchange(back.reshape(ep, -1, quarter), "ep").reshape(slots, quarter)
    tokens_grad = local(combine_kernel, shape((rows, quarter), BF16), "combine", pick, back)

    gate_grad, up_grad = local(
        weight_kernel,
        (shape((tp, quarter, block), BF16), shape((tp, quarter, block), BF16)),
        "weight",
        x,
        grads,
    )
    gate_grad = exchange(gate_grad, "tp").reshape(gate_proj.shape)
    up_grad = exchange(up_grad, "tp").reshape(up_proj.shape)
    down_grad = local(down_kernel, shape((tp, block, quarter), BF16), "down", hid, g)
    down_grad = exchange(down_grad, "tp").transpose(1, 0, 2).reshape(down_proj.shape)

    weights_grad = local(
        functools.partial(share_kernel, cap=cap), shape((top, rows), F32), "share", routes_t, weights_t, share
    )
    weights_grad = lax.psum(weights_grad, "tp").T

    hidden_grad = jnp.dot(cotangent, shared_down, preferred_element_type=F32).astype(BF16)
    shared = lax.dot_general(cotangent, shared_hidden, ROWS, preferred_element_type=F32)
    shared = exchange(shared.astype(BF16).reshape(ep, feat // ep, -1), "ep")
    shared_grad = jnp.sum(shared.astype(F32), axis=0)
    return tokens_grad, weights_grad, gate_grad, up_grad, down_grad, hidden_grad, shared_grad


def solution(mesh):
    return jax.shard_map(
        shards,
        mesh=mesh,
        in_specs=(
            P("ep", None),
            P("ep", None),
            P("ep", None),
            P("ep", None),
            P("ep", None, "tp"),
            P("ep", None, "tp"),
            P("ep", "tp", None),
            P(None, "tp"),
            P("ep", "tp"),
        ),
        out_specs=(
            P("ep", "tp"),
            P("ep", None),
            P("ep", None, "tp"),
            P("ep", None, "tp"),
            P("ep", "tp", None),
            P("ep", "tp"),
            P("ep", "tp"),
        ),
        check_vma=False,
    )
```

```python
import jax
import jax.numpy as jnp
from jax import lax
from jax.experimental import pallas as pl
from jax.experimental.pallas import tpu as pltpu
from jax.sharding import PartitionSpec as P

F32 = jnp.float32
BF16 = jnp.bfloat16
COLS = (((1,), (0,)), ((), ()))
ROWS = (((0,), (0,)), ((), ()))
LAST = (((1,), (1,)), ((), ()))
VMEM = pl.BlockSpec(memory_space=pltpu.VMEM)
SMEM = pl.BlockSpec(memory_space=pltpu.SMEM)
LIMIT = pltpu.CompilerParams(vmem_limit_bytes=20 * 2**20)
CAP = 4
PAD = 16


def mm(a, b, dims=COLS):
    return lax.dot_general(a, b, dims, preferred_element_type=F32)


def around(array, axis):
    size = lax.axis_size(axis)
    arrays = array if isinstance(array, (list, tuple)) else [array] * (size - 1)
    return [
        lax.ppermute(part, axis, [(i, (i + k + 1) % size) for i in range(size)])
        for k, part in enumerate(arrays)
    ]


def at(col, step, parts):
    return lax.rem(col[0] + (step + parts), parts)


def span(index, width):
    return pl.ds(pl.multiple_of(index * width, width), width)


def local(kernel, out, *args, smem=0, scratch=()):
    return pl.pallas_call(
        kernel,
        in_specs=[SMEM] * smem + [VMEM] * (len(args) - smem),
        out_specs=jax.tree.map(lambda _: VMEM, out),
        out_shape=out,
        scratch_shapes=scratch,
        compiler_params=LIMIT,
    )(*args)


def weave():
    rows = 64 * CAP
    row = lax.broadcasted_iota(jnp.int32, (rows, rows), 0)
    col = lax.broadcasted_iota(jnp.int32, (rows, rows), 1)
    s, rest = row // (2 * CAP), row % (2 * CAP)
    h, r = rest // CAP, rest % CAP
    return jnp.where(col == h * (rows // 2) + s * CAP + r, 1.0, 0.0).astype(BF16)


def chosen(routes_ref, slots):
    count = routes_ref.shape[1]
    row = lax.broadcasted_iota(jnp.int32, (slots, count), 0)
    expert = row // CAP
    first = expert == routes_ref[0:1, :]
    second = expert == routes_ref[1:2, :]
    named = jnp.where(first | second, 1.0, 0.0)
    earlier = lax.broadcasted_iota(jnp.int32, (count, count), 0)
    later = lax.broadcasted_iota(jnp.int32, (count, count), 1)
    before = jnp.where(earlier < later, 1.0, 0.0).astype(BF16)
    rank = mm(named.astype(BF16), before)
    place = (row - expert * CAP).astype(F32)
    hit = jnp.where(rank == place, named, 0.0)
    return hit, jnp.where(first, hit, 0.0), jnp.where(second, hit, 0.0)


def dispatch_kernel(col, routes_ref, weights_ref, tok_ref, cot_ref, sent_ref, pick_ref):
    slots = pick_ref.shape[0]
    hit, one, two = chosen(routes_ref, slots)
    weights = weights_ref[...].astype(BF16).astype(F32)
    weight = jnp.sum(one * weights[0:1, :] + two * weights[1:2, :], axis=1, keepdims=True)
    pick = hit.astype(BF16)
    pick_ref[...] = pick
    x = mm(pick, tok_ref[...]).astype(BF16)
    g = (weight * mm(pick, cot_ref[...])).astype(BF16)
    order = weave()
    half = order.shape[0] // 2
    for b in range(slots // half):
        both = jnp.concatenate([x[b * half : (b + 1) * half], g[b * half : (b + 1) * half]], axis=0)
        sent_ref[2 * b * half : 2 * (b + 1) * half, :] = mm(order, both).astype(BF16)


def dispatch(col, routes, weights, tokens, cotangent, slots, quarter):
    rows = tokens.shape[0]
    whole = lambda *shape: pl.BlockSpec(shape, lambda i, col: (0,) * len(shape))
    part = pl.BlockSpec((rows, quarter), lambda i, col: (0, col[0]))
    return pl.pallas_call(
        dispatch_kernel,
        grid_spec=pltpu.PrefetchScalarGridSpec(
            num_scalar_prefetch=1,
            grid=(1,),
            in_specs=[whole(*routes.shape), whole(*weights.shape), part, part],
            out_specs=[whole(2 * slots, quarter), whole(slots, rows)],
        ),
        out_shape=[
            jax.ShapeDtypeStruct((2 * slots, quarter), BF16),
            jax.ShapeDtypeStruct((slots, rows), BF16),
        ],
        compiler_params=LIMIT,
        name="dispatch",
    )(col, routes, weights, tokens, cotangent)


def pack_kernel(col, gate_ref, up_ref, down_ref, *outs):
    parts = len(outs)
    quarter = gate_ref.shape[0] // parts
    block = gate_ref.shape[1]
    for k, out in enumerate(outs):
        to = at(col, k, parts)
        out[:quarter, :] = gate_ref[span(to, quarter), :]
        out[quarter : 2 * quarter, :] = up_ref[span(to, quarter), :]
        down = down_ref[:, span(to, quarter)]
        for c in range(quarter // block):
            row = 2 * quarter + c * block
            out[row : row + block, :] = down[:, c * block : (c + 1) * block]


def collect_kernel(col, *refs):
    *packed, both_ref, down_ref = refs
    parts = len(packed)
    quarter, width = both_ref.shape
    hidden = width // 2
    block = hidden // parts
    for k, ref in enumerate(packed):
        place = span(at(col, -k, parts), block)
        both_ref[:, place] = ref[:quarter, :]
        both_ref[:, span(at(col, -k, parts) + parts, block)] = ref[quarter : 2 * quarter, :]
        for c in range(quarter // block):
            row = 2 * quarter + c * block
            down_ref[place, c * block : (c + 1) * block] = ref[row : row + block, :]


def partial_kernel(col, got_ref, both_ref, down_ref, x_ref, g_ref, *refs):
    *outs, y_ref = refs
    parts = len(outs)
    width = both_ref.shape[1]
    order = weave()
    half = order.shape[0] // 2
    for b in range(got_ref.shape[0] // (2 * half)):
        split = mm(order, got_ref[2 * b * half : 2 * (b + 1) * half, :], ROWS).astype(BF16)
        x_ref[b * half : (b + 1) * half, :] = split[:half]
        g_ref[b * half : (b + 1) * half, :] = split[half:]
    y_ref[:, :width] = mm(x_ref[...], both_ref[...]).astype(BF16)
    y_ref[:, width:] = mm(g_ref[...], down_ref[...], LAST).astype(BF16)
    for k, out in enumerate(outs):
        out[...] = y_ref[span(at(col, k, parts), out.shape[0]), :]


def middle_kernel(col, *refs):
    *parts, grads_ref, share_ref = refs
    rows, width = grads_ref.shape
    hidden = width // 3
    total = parts[0][...].astype(F32)
    for ref in parts[1:]:
        total = total + ref[...].astype(F32)
    gate = total[:, :hidden]
    upper = total[:, hidden : 2 * hidden]
    backed = total[:, 2 * hidden :]
    sigma = jax.nn.sigmoid(gate)
    active = gate * sigma
    hid = (active * upper).astype(BF16)
    grads_ref[:, :hidden] = (backed * upper * sigma * (1.0 + gate * (1.0 - sigma))).astype(BF16)
    grads_ref[:, hidden : 2 * hidden] = (backed * active).astype(BF16)
    grads_ref[:, 2 * hidden :] = hid
    share = jnp.sum(hid.astype(F32) * backed, axis=1, keepdims=True)
    share = jnp.broadcast_to(share, (rows, share_ref.shape[1]))
    for k in range(len(parts)):
        share_ref[k * rows : (k + 1) * rows, :] = jnp.where(col[0] == k, share, 0.0).astype(BF16)


def input_kernel(col, *refs):
    *grads, both_ref, out_ref = refs
    parts = len(grads)
    rows = grads[0].shape[0]
    width = both_ref.shape[1]
    whole = jnp.concatenate([ref[:, :width] for ref in grads], axis=0)
    out = mm(whole, both_ref[...], LAST).astype(BF16)
    order = weave()
    half = out.shape[1] // 2
    for k in range(parts):
        own = out[k * rows : (k + 1) * rows]
        both = jnp.concatenate([own[:, :half], own[:, half:]], axis=0)
        out_ref[span(at(col, -k, parts), 2 * rows), :] = mm(order, both).astype(BF16)


def weight_kernel(col, x_ref, g_ref, routes_ref, weights_ref, share_ref, *refs):
    refs, all_ref, down_ref = refs[:-2], refs[-2], refs[-1]
    parts = len(refs) // 2
    grads, outs = refs[:parts], refs[parts:]
    rows = grads[0].shape[0]
    quarter, width = all_ref.shape
    block = outs[0].shape[1]
    order = [span(at(col, -k, parts), rows) for k in range(parts)]
    x = jnp.concatenate([x_ref[place, :] for place in order], axis=0)
    g = jnp.concatenate([g_ref[place, :] for place in order], axis=0)
    whole = jnp.concatenate([ref[...] for ref in grads], axis=0)
    all_ref[...] = mm(x, whole[:, :width], ROWS).astype(BF16)
    down_ref[...] = mm(whole[:, width:], g, ROWS).astype(BF16)
    _, one, two = chosen(routes_ref, share_ref.shape[0])
    share = share_ref[...].astype(F32)
    weights = weights_ref[...].astype(BF16).astype(F32)
    one = jnp.sum(one * share, axis=0, keepdims=True) / weights[0:1, :]
    two = jnp.sum(two * share, axis=0, keepdims=True) / weights[1:2, :]
    row = lax.broadcasted_iota(jnp.int32, (PAD, block), 0)
    share = jnp.where(row == 0, one, jnp.where(row == 1, two, 0.0)).astype(BF16)
    for k, out in enumerate(outs):
        to = at(col, k, parts)
        out[:quarter, :] = all_ref[:, span(to, block)]
        out[quarter : 2 * quarter, :] = all_ref[:, span(to + parts, block)]
        for c in range(quarter // block):
            row = 2 * quarter + c * block
            out[row : row + block, :] = down_ref[span(to, block), c * block : (c + 1) * block]
        out[3 * quarter :, :] = share


def finish_kernel(col, *refs):
    *got, gate_ref, up_ref, down_ref, share_ref = refs
    parts = len(got)
    block = gate_ref.shape[1]
    quarter = gate_ref.shape[0] // parts
    share = jnp.zeros(share_ref.shape, F32)
    for k, ref in enumerate(got):
        place = span(at(col, -k, parts), quarter)
        gate_ref[place, :] = ref[:quarter, :]
        up_ref[place, :] = ref[quarter : 2 * quarter, :]
        pieces = [ref[row : row + block, :] for row in range(2 * quarter, 3 * quarter, block)]
        down_ref[:, place] = jnp.concatenate(pieces, axis=1)
        share = share + ref[3 * quarter :, :].astype(F32)[: share.shape[0]]
    share_ref[...] = share


def combine_kernel(pick_ref, back_ref, out_ref):
    slots = pick_ref.shape[0]
    order = weave()
    half = order.shape[0] // 2
    left, right = [], []
    for b in range(slots // half):
        own = mm(order, back_ref[2 * b * half : 2 * (b + 1) * half, :], ROWS).astype(BF16)
        left.append(own[:half])
        right.append(own[half:])
    width = back_ref.shape[1]
    pick = pick_ref[...]
    out_ref[:, :width] = mm(pick, jnp.concatenate(left, axis=0), ROWS).astype(BF16)
    out_ref[:, width:] = mm(pick, jnp.concatenate(right, axis=0), ROWS).astype(BF16)


def experts(
    tokens,
    cotangent,
    route_weights,
    routes,
    gate_proj,
    up_proj,
    down_proj,
    shared_down,
    shared_hidden,
):
    rows, feat = tokens.shape
    top = routes.shape[1]
    ep = lax.axis_size("ep")
    tp = lax.axis_size("tp")
    slots = ep * CAP
    quarter = feat // tp
    block = gate_proj.shape[2]
    hidden = block * tp
    some = slots // tp
    half = lambda *shape: jax.ShapeDtypeStruct(shape, BF16)
    over_ep = lambda a: lax.all_to_all(
        a.reshape(ep, -1, a.shape[-1]), "ep", split_axis=0, concat_axis=0, tiled=True
    ).reshape(a.shape)
    col = lax.axis_index("tp").astype(jnp.int32).reshape(1)
    routes_t = routes.T
    weights_t = route_weights.T

    sent, pick = dispatch(col, routes_t, weights_t, tokens, cotangent, slots, quarter)
    got = over_ep(sent)

    packed = local(
        pack_kernel,
        [half(3 * quarter, block)] * tp,
        col,
        gate_proj.reshape(feat, block),
        up_proj.reshape(feat, block),
        down_proj.reshape(block, feat),
        smem=1,
    )
    packed = [packed[0], *around(packed[1:], "tp")]
    both, down = local(
        collect_kernel, [half(quarter, 2 * hidden), half(hidden, quarter)], col, *packed, smem=1
    )

    x, g, *part = local(
        partial_kernel,
        [half(slots, quarter)] * 2 + [half(some, 3 * hidden)] * tp,
        col,
        got,
        both,
        down,
        smem=1,
        scratch=[pltpu.VMEM((slots, 3 * hidden), BF16)],
    )
    part = [part[0], *around(part[1:], "tp")]
    grads, share = local(
        middle_kernel, [half(some, 3 * hidden), half(slots, rows)], col, *part, smem=1
    )
    grads = [grads, *around(grads, "tp")]
    share = over_ep(share)

    back = local(input_kernel, half(2 * slots, quarter // 2), col, *grads, both, smem=1)
    back = over_ep(back)
    tokens_grad = local(combine_kernel, half(rows, quarter), pick, back)

    outer = local(
        weight_kernel,
        [half(3 * quarter + PAD, block)] * tp,
        col,
        x,
        g,
        routes_t,
        weights_t,
        share,
        *grads,
        smem=1,
        scratch=[pltpu.VMEM((quarter, 2 * hidden), BF16), pltpu.VMEM((hidden, quarter), BF16)],
    )
    outer = [outer[0], *around(outer[1:], "tp")]
    gate_grad, up_grad, down_grad, weights_grad = local(
        finish_kernel,
        [half(feat, block)] * 2 + [half(block, feat), jax.ShapeDtypeStruct((top, rows), F32)],
        col,
        *outer,
        smem=1,
    )
    weights_grad = weights_grad.T

    hidden_grad = jnp.dot(cotangent, shared_down, preferred_element_type=F32).astype(BF16)
    shared = lax.dot_general(cotangent, shared_hidden, ROWS, preferred_element_type=F32)
    shared = shared.astype(BF16)
    shared = over_ep(shared)
    shared_grad = jnp.sum(shared.reshape(ep, feat // ep, -1).astype(F32), axis=0)
    return (
        tokens_grad,
        weights_grad,
        gate_grad.reshape(gate_proj.shape),
        up_grad.reshape(up_proj.shape),
        down_grad.reshape(down_proj.shape),
        hidden_grad,
        shared_grad,
    )


def solution(mesh):
    return jax.shard_map(
        experts,
        mesh=mesh,
        in_specs=(
            P("ep", None),
            P("ep", None),
            P("ep", None),
            P("ep", None),
            P("ep", None, "tp"),
            P("ep", None, "tp"),
            P("ep", "tp", None),
            P(None, "tp"),
            P("ep", "tp"),
        ),
        out_specs=(
            P("ep", "tp"),
            P("ep", None),
            P("ep", None, "tp"),
            P("ep", None, "tp"),
            P("ep", "tp", None),
            P("ep", "tp"),
            P("ep", "tp"),
        ),
        check_vma=False,
    )
```

```python
import functools

import jax
import jax.numpy as jnp
from jax import lax
from jax.experimental import pallas as pl
from jax.experimental.pallas import tpu as pltpu
from jax.sharding import Mesh
from jax.sharding import PartitionSpec as P

EP = ("z", "y", "core")
F32 = jnp.float32
BF16 = jnp.bfloat16
COLS = (((1,), (0,)), ((), ()))
ROWS = (((0,), (0,)), ((), ()))
LAST = (((1,), (1,)), ((), ()))
VMEM = pl.BlockSpec(memory_space=pltpu.VMEM)
SMEM = pl.BlockSpec(memory_space=pltpu.SMEM)
HBM = pl.BlockSpec(memory_space=pltpu.HBM)
LIMIT = pltpu.CompilerParams(vmem_limit_bytes=12 * 2**20)
CAP = 4
LANES = 128
FAR = 2
NEAR = (1, 3)
GROUP = 16


def mm(a, b, dims=COLS):
    return lax.dot_general(a, b, dims, preferred_element_type=F32)


def around(array):
    size = lax.axis_size("tp")
    arrays = array if isinstance(array, (list, tuple)) else [array] * (size - 1)
    got = []
    for k, part in enumerate(arrays):
        got.append(lax.ppermute(part, "tp", [(i, (i + k + 1) % size) for i in range(size)]))
    return got


def over(array, axes):
    size = lax.axis_size(axes)
    rows = array.reshape(size, -1, array.shape[-1])
    return lax.all_to_all(rows, axes, split_axis=0, concat_axis=0, tiled=True).reshape(array.shape)


def at(col, step, parts):
    return lax.rem(col[0] + (step + parts), parts)


def span(index, width):
    return pl.ds(pl.multiple_of(index * width, width), width)


def local(kernel, out, *args, spaces="", outs="", scratch=(), alias=None):
    spec = {"s": SMEM, "v": VMEM, "h": HBM}
    kept = {"h": pltpu.HBM}
    spaces = spaces + "v" * (len(args) - len(spaces))
    args = [
        pltpu.with_memory_space_constraint(a, kept[k]) if k in kept else a
        for a, k in zip(args, spaces)
    ]
    single = not isinstance(out, (list, tuple))
    out = [out] if single else list(out)
    outs = outs + "v" * (len(out) - len(outs))
    out = [kept[k](o.shape, o.dtype) if k in kept else o for o, k in zip(out, outs)]
    got = pl.pallas_call(
        kernel,
        in_specs=[spec[k] for k in spaces],
        out_specs=[spec[k] for k in outs],
        out_shape=out,
        scratch_shapes=scratch,
        input_output_aliases=alias or {},
        compiler_params=LIMIT,
    )(*args)
    return got[0] if single else got


def weave():
    rows = 64 * CAP
    row = lax.broadcasted_iota(jnp.int32, (rows, rows), 0)
    col = lax.broadcasted_iota(jnp.int32, (rows, rows), 1)
    s, rest = row // (2 * CAP), row % (2 * CAP)
    h, r = rest // CAP, rest % CAP
    return jnp.where(col == h * (rows // 2) + s * CAP + r, 1.0, 0.0).astype(BF16)


def chosen(routes_ref, slots):
    count = routes_ref.shape[1]
    row = lax.broadcasted_iota(jnp.int32, (slots, count), 0)
    expert = row // CAP
    first = expert == routes_ref[0:1, :]
    second = expert == routes_ref[1:2, :]
    named = jnp.where(first | second, 1.0, 0.0)
    earlier = lax.broadcasted_iota(jnp.int32, (count, count), 0)
    later = lax.broadcasted_iota(jnp.int32, (count, count), 1)
    before = jnp.where(earlier < later, 1.0, 0.0).astype(BF16)
    rank = mm(named.astype(BF16), before)
    place = (row - expert * CAP).astype(F32)
    hit = jnp.where(rank == place, named, 0.0)
    return hit, jnp.where(first, hit, 0.0), jnp.where(second, hit, 0.0)


def dispatch_kernel(
    col, routes_ref, weights_ref, tok_ref, cot_ref, sent_ref, routes, weights, tok, cot, sent, sems
):
    slots = sent_ref.shape[0] // 2
    place = span(col[0], tok.shape[1])
    copies = [
        pltpu.make_async_copy(src, dst, sems.at[k])
        for k, (src, dst) in enumerate(
            [
                (routes_ref, routes),
                (weights_ref, weights),
                (tok_ref.at[:, place], tok),
                (cot_ref.at[:, place], cot),
            ]
        )
    ]
    for copy in copies:
        copy.start()
    order = weave()
    copies[0].wait()
    hit, one, two = chosen(routes, slots)
    pick = hit.astype(BF16)
    copies[1].wait()
    scale = weights[...].astype(BF16).astype(F32)
    weight = jnp.sum(one * scale[0:1, :] + two * scale[1:2, :], axis=1, keepdims=True)
    copies[2].wait()
    x = mm(pick, tok[...]).astype(BF16)
    copies[3].wait()
    g = (weight * mm(pick, cot[...])).astype(BF16)
    half = order.shape[0] // 2
    leaving = []
    for b in range(slots // half):
        both = jnp.concatenate([x[b * half : (b + 1) * half], g[b * half : (b + 1) * half]], axis=0)
        rows = slice(2 * b * half, 2 * (b + 1) * half)
        sent[rows, :] = mm(order, both).astype(BF16)
        leaving.append(
            pltpu.make_async_copy(sent.at[rows, :], sent_ref.at[rows, :], sems.at[4 + b])
        )
        leaving[-1].start()
    for copy in leaving:
        copy.wait()


def pick_kernel(routes_ref, weights_ref, one_ref, two_ref, inverse_ref):
    _, one, two = chosen(routes_ref, one_ref.shape[0])
    one_ref[...] = one.astype(BF16)
    two_ref[...] = two.astype(BF16)
    inverse_ref[...] = 1.0 / weights_ref[...].astype(BF16).astype(F32)


def dots_kernel(cot_ref, hid_ref, down_ref, grad_ref, terms_ref):
    cot = cot_ref[...]
    grad_ref[...] = mm(cot, down_ref[...]).astype(BF16)
    terms = mm(cot, hid_ref[...], ROWS).astype(BF16)
    inner, outer, group, width = terms_ref.shape
    terms = terms.reshape(outer, inner, group, width)
    for k in range(outer):
        terms_ref[:, k] = terms[k]


def fold_kernel(terms_ref, out_ref):
    terms = terms_ref[...].astype(F32)
    out_ref[...] = jnp.sum(terms.reshape(-1, *out_ref.shape), axis=0).astype(BF16)


def total_kernel(terms_ref, out_ref):
    rows, width = terms_ref.shape
    terms = terms_ref[...].astype(F32).reshape(rows // GROUP, GROUP, width)
    out_ref[...] = jnp.sum(terms, axis=0)


def pack_kernel(col, gate_ref, up_ref, down_ref, own_out, *refs):
    *outs, own_ref, sem = refs
    parts = len(outs) + 1
    quarter = gate_ref.shape[0] // parts
    block = gate_ref.shape[1]
    own_copy = pltpu.make_async_copy(own_ref, own_out, sem)
    for k, out in enumerate([own_ref, *outs]):
        to = at(col, k, parts)
        out[:quarter, :] = gate_ref[span(to, quarter), :]
        out[quarter : 2 * quarter, :] = up_ref[span(to, quarter), :]
        down = down_ref[:, span(to, quarter)]
        for c in range(quarter // block):
            row = 2 * quarter + c * block
            out[row : row + block, :] = down[:, c * block : (c + 1) * block]
        if k == 0:
            own_copy.start()
    own_copy.wait()


def collect_kernel(col, own_ref, *refs):
    *packed, both_ref, down_ref, sems = refs
    parts = len(packed) + 1
    quarter, width = both_ref.shape
    block = width // (2 * parts)
    copies = []
    for k, ref in enumerate([own_ref, *packed]):
        index = at(col, -k, parts)
        place = span(index, block)
        pairs = [
            (slice(0, quarter), both_ref.at[:, place]),
            (slice(quarter, 2 * quarter), both_ref.at[:, span(index + parts, block)]),
        ]
        for c in range(quarter // block):
            row = 2 * quarter + c * block
            across = slice(c * block, (c + 1) * block)
            pairs.append((slice(row, row + block), down_ref.at[place, across]))
        for rows, out in pairs:
            if k == 0:
                copies.append(pltpu.make_async_copy(ref.at[rows, :], out, sems.at[len(copies)]))
                copies[-1].start()
            else:
                out[...] = ref[rows, :]
    for copy in copies:
        copy.wait()


def apart(order, got):
    split = mm(order, got, ROWS).astype(BF16)
    half = split.shape[0] // 2
    return split[:half], split[half:]


def far_kernel(col, got_ref, both_ref, down_ref, out_ref):
    rows = out_ref.shape[0]
    parts = got_ref.shape[0] // (2 * rows)
    width = both_ref.shape[1]
    x, g = apart(weave(), got_ref[span(at(col, FAR, parts), 2 * rows), :])
    out_ref[:, :width] = mm(x, both_ref[...]).astype(BF16)
    out_ref[:, width:] = mm(g, down_ref[...], LAST).astype(BF16)


def near_kernel(col, got_ref, both_ref, down_ref, xg_out, own_out, *refs):
    *outs, xg_ref, own_ref, sems = refs
    rows = own_ref.shape[0]
    parts = got_ref.shape[0] // (2 * rows)
    width = both_ref.shape[1]
    quarter = got_ref.shape[1]
    order = weave()
    for b in range(parts):
        x, g = apart(order, got_ref[2 * b * rows : 2 * (b + 1) * rows, :])
        xg_ref[b * rows : (b + 1) * rows, :quarter] = x
        xg_ref[b * rows : (b + 1) * rows, quarter:] = g
    xg_copy = pltpu.make_async_copy(xg_ref, xg_out, sems.at[0])
    xg_copy.start()
    blocks = [span(at(col, k, parts), rows) for k in [0, *NEAR]]
    xg = jnp.concatenate([xg_ref[place, :] for place in blocks], axis=0)
    grown = mm(xg[:, :quarter], both_ref[...]).astype(BF16)
    backed = mm(xg[:, quarter:], down_ref[...], LAST).astype(BF16)
    own_copy = pltpu.make_async_copy(own_ref, own_out, sems.at[1])
    for k, out in enumerate([own_ref, *outs]):
        out[:, :width] = grown[k * rows : (k + 1) * rows]
        out[:, width:] = backed[k * rows : (k + 1) * rows]
        if k == 0:
            own_copy.start()
    xg_copy.wait()
    own_copy.wait()


def middle_kernel(*refs):
    *parts, grads_ref = refs
    rows, width = parts[0].shape
    hidden = width // 3
    total = parts[0][...].astype(F32)
    for ref in parts[1:]:
        total = total + ref[...].astype(F32)
    gate = total[:, :hidden]
    upper = total[:, hidden : 2 * hidden]
    backed = total[:, 2 * hidden :]
    sigma = jax.nn.sigmoid(gate)
    active = gate * sigma
    hid = (active * upper).astype(BF16)
    grads_ref[:, :hidden] = (backed * upper * sigma * (1.0 + gate * (1.0 - sigma))).astype(BF16)
    grads_ref[:, hidden : 2 * hidden] = (backed * active).astype(BF16)
    grads_ref[:, 2 * hidden : width] = hid
    share = jnp.sum(hid.astype(F32) * backed, axis=1, keepdims=True)
    grads_ref[:, width:] = jnp.broadcast_to(share, (rows, LANES)).astype(BF16)


def input_kernel(col, *refs):
    *grads, both_ref, back_out, out_ref, sems = refs
    parts = len(grads)
    rows = grads[0].shape[0]
    width = both_ref.shape[1]
    whole = jnp.concatenate([ref[:, :width] for ref in grads], axis=0)
    out = mm(whole, both_ref[...], LAST).astype(BF16)
    order = weave()
    half = out.shape[1] // 2
    copies = []
    for k, ref in enumerate(grads):
        own = out[k * rows : (k + 1) * rows]
        both = jnp.concatenate([own[:, :half], own[:, half:]], axis=0)
        place = slice(2 * k * rows, 2 * (k + 1) * rows)
        out_ref[place, :half] = mm(order, both).astype(BF16)
        share = ref[:, ref.shape[1] - LANES :]
        out_ref[place, half:] = mm(order[:, :rows], share).astype(BF16)
        to = back_out.at[span(at(col, -k, parts), 2 * rows), :]
        copies.append(pltpu.make_async_copy(out_ref.at[place, :], to, sems.at[k]))
        copies[-1].start()
    for copy in copies:
        copy.wait()


def outer_terms(col, steps, xg_ref, grads):
    parts = len(grads)
    rows = grads[0].shape[0]
    block = (grads[0].shape[1] - LANES) // (3 * parts)
    quarter = xg_ref.shape[1] // 2
    order = [span(at(col, -k, parts), rows) for k in range(parts)]
    x = jnp.concatenate([xg_ref[place, :quarter] for place in order], axis=0)
    g = jnp.concatenate([xg_ref[place, quarter:] for place in order], axis=0)

    def units(kinds):
        places = [span(at(col, k, parts) + kind * parts, block) for k in steps for kind in kinds]
        return jnp.concatenate(
            [jnp.concatenate([ref[:, place] for place in places], axis=1) for ref in grads], axis=0
        )

    both = mm(x, units((0, 1)), ROWS).astype(BF16)
    down = mm(units((2,)), g, ROWS).astype(BF16)
    return [
        (
            both[:, 2 * n * block : (2 * n + 1) * block],
            both[:, (2 * n + 1) * block : (2 * n + 2) * block],
            down[n * block : (n + 1) * block],
        )
        for n in range(len(steps))
    ]


def outer_kernel(col, xg_ref, *refs, steps):
    grads, outs = refs[: -len(steps)], refs[-len(steps) :]
    for out, (gate, up, down) in zip(outs, outer_terms(col, steps, xg_ref, grads)):
        quarter, block = gate.shape
        out[:quarter, :] = gate
        out[quarter : 2 * quarter, :] = up
        for c in range(quarter // block):
            row = 2 * quarter + c * block
            out[row : row + block, :] = down[:, c * block : (c + 1) * block]


def own_kernel(col, xg_ref, *refs):
    *grads, gate_out, up_out, down_out, gate_ref, up_ref, down_ref, sems = refs
    place = span(at(col, 0, len(grads)), gate_ref.shape[0])
    [(gate, up, down)] = outer_terms(col, (0,), xg_ref, grads)
    gate_ref[...] = gate
    up_ref[...] = up
    down_ref[...] = down
    copies = [
        pltpu.make_async_copy(gate_ref, gate_out.at[place, :], sems.at[0]),
        pltpu.make_async_copy(up_ref, up_out.at[place, :], sems.at[1]),
        pltpu.make_async_copy(down_ref, down_out.at[:, place], sems.at[2]),
    ]
    for copy in copies:
        copy.start()
    for copy in copies:
        copy.wait()


def finish_kernel(col, *refs):
    *refs, sems = refs
    parts = len(refs) - 5
    got, (gate_ref, up_ref, down_ref) = refs[: parts - 1], refs[parts + 2 :]
    block = gate_ref.shape[1]
    quarter = gate_ref.shape[0] // parts
    copies = []
    for k, ref in enumerate(got):
        index = at(col, -k - 1, parts)
        place = span(index, quarter)
        pairs = [
            (ref.at[:quarter, :], gate_ref.at[place, :]),
            (ref.at[quarter : 2 * quarter, :], up_ref.at[place, :]),
        ]
        for c in range(quarter // block):
            row = 2 * quarter + c * block
            across = span(index * (quarter // block) + c, block)
            pairs.append((ref.at[row : row + block, :], down_ref.at[:, across]))
        for src, dst in pairs:
            copies.append(pltpu.make_async_copy(src, dst, sems.at[len(copies)]))
            copies[-1].start()
    for copy in copies:
        copy.wait()


def combine_kernel(inverse_ref, one_ref, two_ref, back_ref, out_ref, weights_out):
    slots = one_ref.shape[0]
    order = weave()
    half = order.shape[0] // 2
    width = out_ref.shape[1] // 2
    left, right, shares = [], [], []
    for b in range(slots // half):
        own = mm(order, back_ref[2 * b * half : 2 * (b + 1) * half, :], ROWS).astype(BF16)
        left.append(own[:half, :width])
        right.append(own[half:, :width])
        shares.append(own[:half, width:].astype(F32))
    one = one_ref[...]
    two = two_ref[...]
    pick = one + two
    out_ref[:, :width] = mm(pick, jnp.concatenate(left, axis=0), ROWS).astype(BF16)
    out_ref[:, width:] = mm(pick, jnp.concatenate(right, axis=0), ROWS).astype(BF16)
    share = jnp.concatenate(shares, axis=0)
    for k, mask in enumerate([one, two]):
        total = jnp.sum(mask.astype(F32) * share, axis=0, keepdims=True)
        weights_out[k : k + 1, :] = total * inverse_ref[k : k + 1, :]


def experts(
    tokens,
    cotangent,
    route_weights,
    routes,
    gate_proj,
    up_proj,
    down_proj,
    shared_down,
    shared_hidden,
):
    rows, feat = tokens.shape
    top = routes.shape[1]
    ep = lax.axis_size(EP)
    tp = lax.axis_size("tp")
    slots = ep * CAP
    quarter = feat // tp
    block = gate_proj.shape[2]
    hidden = block * tp
    some = slots // tp
    half = lambda *shape: jax.ShapeDtypeStruct(shape, BF16)
    col = lax.axis_index("tp").astype(jnp.int32).reshape(1)
    routes_t = routes.T
    weights_t = route_weights.T

    sent = local(
        dispatch_kernel,
        half(2 * slots, quarter),
        col,
        routes_t,
        weights_t,
        tokens,
        cotangent,
        spaces="shhhh",
        outs="h",
        scratch=[
            pltpu.VMEM(routes_t.shape, jnp.int32),
            pltpu.VMEM(weights_t.shape, F32),
            pltpu.VMEM((rows, quarter), BF16),
            pltpu.VMEM((rows, quarter), BF16),
            pltpu.VMEM((2 * slots, quarter), BF16),
            pltpu.SemaphoreType.DMA((4 + tp,)),
        ],
    )
    got = over(sent, EP)

    packed = local(
        pack_kernel,
        [half(3 * quarter, block)] * tp,
        col,
        gate_proj.reshape(feat, block),
        up_proj.reshape(feat, block),
        down_proj.reshape(block, feat),
        spaces="s",
        outs="h",
        scratch=[pltpu.VMEM((3 * quarter, block), BF16), pltpu.SemaphoreType.DMA],
    )
    packed = [packed[0], *around(packed[1:])]
    both, down = local(
        collect_kernel,
        [half(quarter, 2 * hidden), half(hidden, quarter)],
        col,
        *packed,
        spaces="sh",
        scratch=[pltpu.SemaphoreType.DMA((2 + tp,))],
    )

    far = local(far_kernel, half(some, 3 * hidden), col, got, both, down, spaces="s")
    xg, own, *near = local(
        near_kernel,
        [half(slots, 2 * quarter)] + [half(some, 3 * hidden)] * (1 + len(NEAR)),
        col,
        got,
        both,
        down,
        spaces="s",
        outs="hh",
        scratch=[
            pltpu.VMEM((slots, 2 * quarter), BF16),
            pltpu.VMEM((some, 3 * hidden), BF16),
            pltpu.SemaphoreType.DMA((2,)),
        ],
    )
    part = [own, *around([near[0], far, near[1]])]
    grads = local(middle_kernel, half(some, 3 * hidden + LANES), *part)
    grads = [grads, *around(grads)]

    back = local(
        input_kernel,
        half(2 * slots, quarter // 2 + LANES),
        col,
        *grads,
        both,
        spaces="s",
        outs="h",
        scratch=[
            pltpu.VMEM((2 * slots, quarter // 2 + LANES), BF16),
            pltpu.SemaphoreType.DMA((tp,)),
        ],
    )
    back = over(back, EP)
    one, two, inverse = local(
        pick_kernel,
        [half(slots, rows)] * 2 + [jax.ShapeDtypeStruct((top, rows), F32)],
        routes_t,
        weights_t,
    )
    tokens_grad, weights_grad = local(
        combine_kernel,
        [half(rows, quarter), jax.ShapeDtypeStruct((top, rows), F32)],
        inverse,
        one,
        two,
        back,
    )
    weights_grad = weights_grad.T

    outer = {}
    for steps in ((FAR,), NEAR):
        got = local(
            functools.partial(outer_kernel, steps=steps),
            [half(3 * quarter, block)] * len(steps),
            col,
            xg,
            *grads,
            spaces="s",
        )
        outer.update(zip(steps, got))
    outer = around([outer[k] for k in range(1, tp)])
    whole = [half(feat, block), half(feat, block), half(block, feat)]
    own = local(
        own_kernel,
        whole,
        col,
        xg,
        *grads,
        spaces="s",
        outs="hhh",
        scratch=[
            pltpu.VMEM((quarter, block), BF16),
            pltpu.VMEM((quarter, block), BF16),
            pltpu.VMEM((block, quarter), BF16),
            pltpu.SemaphoreType.DMA((3,)),
        ],
    )
    gate_grad, up_grad, down_grad = local(
        finish_kernel,
        whole,
        col,
        *outer,
        *own,
        spaces="s" + "v" * (tp - 1) + "hhh",
        outs="hhh",
        scratch=[pltpu.SemaphoreType.DMA(((tp - 1) * (2 + tp),))],
        alias={tp: 0, tp + 1: 1, tp + 2: 2},
    )

    inner = ep // lax.axis_size("z")
    group = feat // ep
    hidden_grad, shared = local(
        dots_kernel,
        [half(rows, block), half(inner, ep // inner, group, block)],
        cotangent,
        shared_hidden,
        shared_down,
    )
    shared = over(shared.reshape(feat, block), ("y", "core"))
    shared = local(fold_kernel, half(feat // inner, block), shared)
    shared = over(shared, "z")
    shared_grad = local(
        total_kernel, jax.ShapeDtypeStruct((feat // ep, block), F32), shared
    )
    return (
        tokens_grad,
        weights_grad,
        gate_grad.reshape(gate_proj.shape),
        up_grad.reshape(up_proj.shape),
        down_grad.reshape(down_proj.shape),
        hidden_grad,
        shared_grad,
    )


def solution(mesh):
    devices = mesh.devices
    split = Mesh(devices.reshape(8, -1, 2, devices.shape[-1]), (*EP, "tp"))
    return jax.shard_map(
        experts,
        mesh=split,
        in_specs=(
            P(EP, None),
            P(EP, None),
            P(EP, None),
            P(EP, None),
            P(EP, None, "tp"),
            P(EP, None, "tp"),
            P(EP, "tp", None),
            P(None, "tp"),
            P(EP, "tp"),
        ),
        out_specs=(
            P(EP, "tp"),
            P(EP, None),
            P(EP, None, "tp"),
            P(EP, None, "tp"),
            P(EP, "tp", None),
            P(EP, "tp"),
            P(EP, "tp"),
        ),
        check_vma=False,
    )
```

```python
import functools

import jax
import jax.numpy as jnp
from jax import lax
from jax.experimental import pallas as pl
from jax.experimental.pallas import tpu as pltpu
from jax.sharding import Mesh
from jax.sharding import PartitionSpec as P

EP = ("z", "y", "core")
F32 = jnp.float32
BF16 = jnp.bfloat16
COLS = (((1,), (0,)), ((), ()))
ROWS = (((0,), (0,)), ((), ()))
LAST = (((1,), (1,)), ((), ()))
VMEM = pl.BlockSpec(memory_space=pltpu.VMEM)
SMEM = pl.BlockSpec(memory_space=pltpu.SMEM)
HBM = pl.BlockSpec(memory_space=pltpu.HBM)
LIMIT = pltpu.CompilerParams(vmem_limit_bytes=12 * 2**20)
CAP = 4
LANES = 128
PAD = 16
FAR = 2
NEAR = (1, 3)
GROUP = 16


def mm(a, b, dims=COLS):
    return lax.dot_general(a, b, dims, preferred_element_type=F32)


def around(array):
    size = lax.axis_size("tp")
    arrays = array if isinstance(array, (list, tuple)) else [array] * (size - 1)
    got = []
    for k, part in enumerate(arrays):
        got.append(lax.ppermute(part, "tp", [(i, (i + k + 1) % size) for i in range(size)]))
    return got


def over(array, axes):
    size = lax.axis_size(axes)
    rows = array.reshape(size, -1, array.shape[-1])
    return lax.all_to_all(rows, axes, split_axis=0, concat_axis=0, tiled=True).reshape(array.shape)


def at(col, step, parts):
    return lax.rem(col[0] + (step + parts), parts)


def span(index, width):
    return pl.ds(pl.multiple_of(index * width, width), width)


def local(kernel, out, *args, spaces="", outs="", scratch=(), alias=None):
    spec = {"s": SMEM, "v": VMEM, "h": HBM}
    kept = {"h": pltpu.HBM}
    spaces = spaces + "v" * (len(args) - len(spaces))
    args = [
        pltpu.with_memory_space_constraint(a, kept[k]) if k in kept else a
        for a, k in zip(args, spaces)
    ]
    single = not isinstance(out, (list, tuple))
    out = [out] if single else list(out)
    outs = outs + "v" * (len(out) - len(outs))
    out = [kept[k](o.shape, o.dtype) if k in kept else o for o, k in zip(out, outs)]
    got = pl.pallas_call(
        kernel,
        in_specs=[spec[k] for k in spaces],
        out_specs=[spec[k] for k in outs],
        out_shape=out,
        scratch_shapes=scratch,
        input_output_aliases=alias or {},
        compiler_params=LIMIT,
    )(*args)
    return got[0] if single else got


def weave():
    rows = 64 * CAP
    row = lax.broadcasted_iota(jnp.int32, (rows, rows), 0)
    col = lax.broadcasted_iota(jnp.int32, (rows, rows), 1)
    s, rest = row // (2 * CAP), row % (2 * CAP)
    h, r = rest // CAP, rest % CAP
    return jnp.where(col == h * (rows // 2) + s * CAP + r, 1.0, 0.0).astype(BF16)


def chosen(routes_ref, slots, turns=1, start=0):
    count = routes_ref.shape[1]
    row = start + lax.broadcasted_iota(jnp.int32, (turns * slots, count), 0)
    expert = row // (turns * CAP)
    first = expert == routes_ref[0:1, :]
    second = expert == routes_ref[1:2, :]
    named = jnp.where(first | second, 1.0, 0.0)
    earlier = lax.broadcasted_iota(jnp.int32, (count, count), 0)
    later = lax.broadcasted_iota(jnp.int32, (count, count), 1)
    before = jnp.where(earlier < later, 1.0, 0.0).astype(BF16)
    rank = mm(named.astype(BF16), before)
    place = (row % CAP).astype(F32)
    hit = jnp.where(rank == place, named, 0.0)
    return hit, jnp.where(first, hit, 0.0), jnp.where(second, hit, 0.0)


def dispatch_kernel(
    col, routes_ref, weights_ref, tok_ref, cot_ref, sent_ref, routes, weights, both, sent, sems
):
    slots = sent_ref.shape[0] // 2
    rows, quarter = tok_ref.shape[0], both.shape[1]
    place = span(col[0], quarter)
    copies = [
        pltpu.make_async_copy(src, dst, sems.at[k])
        for k, (src, dst) in enumerate(
            [
                (routes_ref, routes),
                (weights_ref, weights),
                (tok_ref.at[:, place], both.at[:rows, :]),
                (cot_ref.at[:, place], both.at[rows:, :]),
            ]
        )
    ]
    for copy in copies:
        copy.start()
    half = slots // 2
    leaving = []
    for b in range(2 * slots // half):
        if b == 0:
            copies[0].wait()
        hit, one, two = chosen(routes, half // 2, 2, b * half)
        kind = (lax.broadcasted_iota(jnp.int32, hit.shape, 0) // CAP) % 2
        pick = jnp.concatenate(
            [jnp.where(kind == 0, hit, 0.0), jnp.where(kind == 1, hit, 0.0)], axis=1
        )
        if b == 0:
            copies[1].wait()
        scale = weights[...].astype(BF16).astype(F32)
        weight = jnp.sum(one * scale[0:1, :] + two * scale[1:2, :], axis=1, keepdims=True)
        weight = jnp.where(kind[:, 0:1] == 0, 1.0, weight)
        if b == 0:
            copies[2].wait()
            copies[3].wait()
        part = slice(b * half, (b + 1) * half)
        sent[part, :] = (weight * mm(pick.astype(BF16), both[...])).astype(BF16)
        leaving.append(
            pltpu.make_async_copy(sent.at[part, :], sent_ref.at[part, :], sems.at[4 + b])
        )
        leaving[-1].start()
    for copy in leaving:
        copy.wait()


def pick_kernel(routes_ref, weights_ref, one_ref, two_ref, inverse_ref):
    _, one, two = chosen(routes_ref, one_ref.shape[0])
    one_ref[...] = one.astype(BF16)
    two_ref[...] = two.astype(BF16)
    inverse_ref[...] = 1.0 / weights_ref[...].astype(BF16).astype(F32)


def dots_kernel(cot_ref, hid_ref, down_ref, grad_ref, terms_ref):
    cot = cot_ref[...]
    grad_ref[...] = mm(cot, down_ref[...]).astype(BF16)
    terms = mm(cot, hid_ref[...], ROWS).astype(BF16)
    inner, outer, group, width = terms_ref.shape
    terms = terms.reshape(outer, inner, group, width)
    for k in range(outer):
        terms_ref[:, k] = terms[k]


def fold_kernel(terms_hbm, out_ref, terms_ref, sem):
    copy = pltpu.make_async_copy(terms_hbm, terms_ref, sem)
    copy.start()
    copy.wait()
    terms = terms_ref[...].astype(F32)
    out_ref[...] = jnp.sum(terms.reshape(-1, *out_ref.shape), axis=0).astype(BF16)


def total_kernel(terms_ref, out_ref):
    rows, width = terms_ref.shape
    terms = terms_ref[...].astype(F32).reshape(rows // GROUP, GROUP, width)
    out_ref[...] = jnp.sum(terms, axis=0)


def pack_kernel(col, gate_ref, up_ref, down_ref, own_out, *refs):
    *outs, own_ref, sem = refs
    parts = len(outs) + 1
    quarter = gate_ref.shape[0] // parts
    block = gate_ref.shape[1]
    own_copy = pltpu.make_async_copy(own_ref, own_out, sem)
    for k, out in enumerate([own_ref, *outs]):
        to = at(col, k, parts)
        out[:quarter, :] = gate_ref[span(to, quarter), :]
        out[quarter : 2 * quarter, :] = up_ref[span(to, quarter), :]
        down = down_ref[:, span(to, quarter)]
        for c in range(quarter // block):
            row = 2 * quarter + c * block
            out[row : row + block, :] = down[:, c * block : (c + 1) * block]
        if k == 0:
            own_copy.start()
    own_copy.wait()


def collect_kernel(col, own_ref, *refs):
    *packed, both_ref, down_ref, sems = refs
    parts = len(packed) + 1
    quarter, width = both_ref.shape
    block = width // (2 * parts)
    copies = []
    for k, ref in enumerate([own_ref, *packed]):
        index = at(col, -k, parts)
        place = span(index, block)
        pairs = [
            (slice(0, quarter), both_ref.at[:, place]),
            (slice(quarter, 2 * quarter), both_ref.at[:, span(index + parts, block)]),
        ]
        for c in range(quarter // block):
            row = 2 * quarter + c * block
            across = slice(c * block, (c + 1) * block)
            pairs.append((slice(row, row + block), down_ref.at[place, across]))
        for rows, out in pairs:
            if k == 0:
                copies.append(pltpu.make_async_copy(ref.at[rows, :], out, sems.at[len(copies)]))
                copies[-1].start()
            else:
                out[...] = ref[rows, :]
    for copy in copies:
        copy.wait()


def apart(order, got):
    split = mm(order, got, ROWS).astype(BF16)
    half = split.shape[0] // 2
    return split[:half], split[half:]


def far_kernel(col, got_ref, both_ref, down_ref, out_ref):
    rows = out_ref.shape[0]
    parts = got_ref.shape[0] // (2 * rows)
    width = both_ref.shape[1]
    x, g = apart(weave(), got_ref[span(at(col, FAR, parts), 2 * rows), :])
    out_ref[:, :width] = mm(x, both_ref[...]).astype(BF16)
    out_ref[:, width:] = mm(g, down_ref[...], LAST).astype(BF16)


def near_kernel(col, got_ref, both_ref, down_ref, xg_out, own_out, both_out, *refs):
    *outs, xg_ref, own_ref, sems = refs
    both_copy = pltpu.make_async_copy(both_ref, both_out, sems.at[2])
    both_copy.start()
    rows = own_ref.shape[0]
    parts = got_ref.shape[0] // (2 * rows)
    width = both_ref.shape[1]
    quarter = got_ref.shape[1]
    order = weave()
    for b in range(parts):
        x, g = apart(order, got_ref[2 * b * rows : 2 * (b + 1) * rows, :])
        xg_ref[b * rows : (b + 1) * rows, :quarter] = x
        xg_ref[b * rows : (b + 1) * rows, quarter:] = g
    xg_copy = pltpu.make_async_copy(xg_ref, xg_out, sems.at[0])
    xg_copy.start()
    blocks = [span(at(col, k, parts), rows) for k in [0, *NEAR]]
    xg = jnp.concatenate([xg_ref[place, :] for place in blocks], axis=0)
    grown = mm(xg[:, :quarter], both_ref[...]).astype(BF16)
    backed = mm(xg[:, quarter:], down_ref[...], LAST).astype(BF16)
    own_copy = pltpu.make_async_copy(own_ref, own_out, sems.at[1])
    for k, out in enumerate([own_ref, *outs]):
        out[:, :width] = grown[k * rows : (k + 1) * rows]
        out[:, width:] = backed[k * rows : (k + 1) * rows]
        if k == 0:
            own_copy.start()
    xg_copy.wait()
    own_copy.wait()
    both_copy.wait()


def diagonal(size):
    row = lax.broadcasted_iota(jnp.int32, (size, size), 0)
    return row == lax.broadcasted_iota(jnp.int32, (size, size), 1)


def middle_kernel(*refs):
    *parts, grads_ref = refs
    rows, width = parts[0].shape
    hidden = width // 3
    total = parts[0][...].astype(F32)
    for ref in parts[1:]:
        total = total + ref[...].astype(F32)
    gate = total[:, :hidden]
    upper = total[:, hidden : 2 * hidden]
    backed = total[:, 2 * hidden :]
    sigma = jax.nn.sigmoid(gate)
    active = gate * sigma
    hid = (active * upper).astype(BF16)
    d_gate = (backed * upper * sigma * (1.0 + gate * (1.0 - sigma))).astype(BF16)
    d_up = (backed * active).astype(BF16)
    blocks = hidden // LANES
    for k, value in enumerate([d_gate, d_up, hid]):
        for c in range(blocks):
            row = (k * blocks + c) * rows
            grads_ref[row : row + rows, :] = value[:, c * LANES : (c + 1) * LANES]
    share = jnp.sum(hid.astype(F32) * backed, axis=1, keepdims=True)
    share = jnp.sum(jnp.where(diagonal(rows), share, 0.0), axis=0, keepdims=True)
    grads_ref[3 * blocks * rows :, :] = jnp.broadcast_to(share, (PAD, LANES)).astype(BF16)


def ready_kernel(both_hbm, both_ref, sem):
    copy = pltpu.make_async_copy(both_hbm, both_ref, sem)
    copy.start()
    copy.wait()


def input_kernel(col, *refs):
    *grads, both_ref, back_out, out_ref, sems = refs
    parts = len(grads)
    rows = out_ref.shape[0] // (2 * parts)
    blocks = both_ref.shape[1] // LANES
    whole = jnp.concatenate(
        [
            jnp.concatenate([ref[c * rows : (c + 1) * rows, :] for c in range(blocks)], axis=1)
            for ref in grads
        ],
        axis=0,
    )
    out = mm(whole, both_ref[...], LAST).astype(BF16)
    order = weave()
    half = out.shape[1] // 2
    copies = []
    for k, ref in enumerate(grads):
        own = out[k * rows : (k + 1) * rows]
        both = jnp.concatenate([own[:, :half], own[:, half:]], axis=0)
        place = slice(2 * k * rows, 2 * (k + 1) * rows)
        out_ref[place, :half] = mm(order, both).astype(BF16)
        share = ref[ref.shape[0] - PAD :, :].astype(F32)[0:1]
        share = jnp.sum(jnp.where(diagonal(rows), share, 0.0), axis=1, keepdims=True)
        share = jnp.broadcast_to(share, (rows, LANES)).astype(BF16)
        out_ref[place, half:] = mm(order[:, :rows], share).astype(BF16)
        to = back_out.at[span(at(col, -k, parts), 2 * rows), :]
        copies.append(pltpu.make_async_copy(out_ref.at[place, :], to, sems.at[k]))
        copies[-1].start()
    for copy in copies:
        copy.wait()


def outer_terms(col, steps, xg_ref, grads):
    parts = len(grads)
    rows = xg_ref.shape[0] // parts
    block = LANES
    quarter = xg_ref.shape[1] // 2
    order = [span(at(col, -k, parts), rows) for k in range(parts)]
    x = jnp.concatenate([xg_ref[place, :quarter] for place in order], axis=0)
    g = jnp.concatenate([xg_ref[place, quarter:] for place in order], axis=0)

    def units(kinds):
        places = [span(at(col, k, parts) + kind * parts, rows) for k in steps for kind in kinds]
        return jnp.concatenate(
            [jnp.concatenate([ref[place, :] for place in places], axis=1) for ref in grads], axis=0
        )

    both = mm(x, units((0, 1)), ROWS).astype(BF16)
    down = mm(units((2,)), g, ROWS).astype(BF16)
    return [
        (
            both[:, 2 * n * block : (2 * n + 1) * block],
            both[:, (2 * n + 1) * block : (2 * n + 2) * block],
            down[n * block : (n + 1) * block],
        )
        for n in range(len(steps))
    ]


def outer_kernel(col, xg_ref, *refs, steps):
    grads, outs = refs[: -len(steps)], refs[-len(steps) :]
    for out, (gate, up, down) in zip(outs, outer_terms(col, steps, xg_ref, grads)):
        quarter, block = gate.shape
        out[:quarter, :] = gate
        out[quarter : 2 * quarter, :] = up
        for c in range(quarter // block):
            row = 2 * quarter + c * block
            out[row : row + block, :] = down[:, c * block : (c + 1) * block]


def own_kernel(col, xg_ref, *refs):
    *grads, gate_out, up_out, down_out, gate_ref, up_ref, down_ref, sems = refs
    place = span(at(col, 0, len(grads)), gate_ref.shape[0])
    [(gate, up, down)] = outer_terms(col, (0,), xg_ref, grads)
    gate_ref[...] = gate
    up_ref[...] = up
    down_ref[...] = down
    copies = [
        pltpu.make_async_copy(gate_ref, gate_out.at[place, :], sems.at[0]),
        pltpu.make_async_copy(up_ref, up_out.at[place, :], sems.at[1]),
        pltpu.make_async_copy(down_ref, down_out.at[:, place], sems.at[2]),
    ]
    for copy in copies:
        copy.start()
    for copy in copies:
        copy.wait()


def finish_kernel(col, *refs, steps):
    *refs, sems = refs
    got, (gate_ref, up_ref, down_ref) = refs[: len(steps)], refs[-3:]
    block = gate_ref.shape[1]
    quarter = got[0].shape[0] // 3
    parts = gate_ref.shape[0] // quarter
    copies = []
    for k, ref in zip(steps, got):
        index = at(col, -k, parts)
        place = span(index, quarter)
        pairs = [
            (ref.at[:quarter, :], gate_ref.at[place, :]),
            (ref.at[quarter : 2 * quarter, :], up_ref.at[place, :]),
        ]
        for c in range(quarter // block):
            row = 2 * quarter + c * block
            across = span(index * (quarter // block) + c, block)
            pairs.append((ref.at[row : row + block, :], down_ref.at[:, across]))
        for src, dst in pairs:
            copies.append(pltpu.make_async_copy(src, dst, sems.at[len(copies)]))
            copies[-1].start()
    for copy in copies:
        copy.wait()


def combine_kernel(inverse_ref, one_ref, two_ref, back_ref, out_ref, weights_out):
    slots = one_ref.shape[0]
    order = weave()
    half = order.shape[0] // 2
    width = out_ref.shape[1] // 2
    left, right, shares = [], [], []
    for b in range(slots // half):
        own = mm(order, back_ref[2 * b * half : 2 * (b + 1) * half, :], ROWS).astype(BF16)
        left.append(own[:half, :width])
        right.append(own[half:, :width])
        shares.append(own[:half, width:].astype(F32))
    one = one_ref[...]
    two = two_ref[...]
    pick = one + two
    out_ref[:, :width] = mm(pick, jnp.concatenate(left, axis=0), ROWS).astype(BF16)
    out_ref[:, width:] = mm(pick, jnp.concatenate(right, axis=0), ROWS).astype(BF16)
    share = jnp.concatenate(shares, axis=0)
    for k, mask in enumerate([one, two]):
        total = jnp.sum(mask.astype(F32) * share, axis=0, keepdims=True)
        weights_out[k : k + 1, :] = total * inverse_ref[k : k + 1, :]


def experts(
    tokens,
    cotangent,
    route_weights,
    routes,
    gate_proj,
    up_proj,
    down_proj,
    shared_down,
    shared_hidden,
):
    rows, feat = tokens.shape
    top = routes.shape[1]
    ep = lax.axis_size(EP)
    tp = lax.axis_size("tp")
    slots = ep * CAP
    quarter = feat // tp
    block = gate_proj.shape[2]
    hidden = block * tp
    some = slots // tp
    half = lambda *shape: jax.ShapeDtypeStruct(shape, BF16)
    col = lax.axis_index("tp").astype(jnp.int32).reshape(1)
    routes_t = routes.T
    weights_t = route_weights.T

    sent = local(
        dispatch_kernel,
        half(2 * slots, quarter),
        col,
        routes_t,
        weights_t,
        tokens,
        cotangent,
        spaces="shhhh",
        outs="h",
        scratch=[
            pltpu.VMEM(routes_t.shape, jnp.int32),
            pltpu.VMEM(weights_t.shape, F32),
            pltpu.VMEM((2 * rows, quarter), BF16),
            pltpu.VMEM((2 * slots, quarter), BF16),
            pltpu.SemaphoreType.DMA((4 + tp,)),
        ],
    )
    got = over(sent, EP)

    packed = local(
        pack_kernel,
        [half(3 * quarter, block)] * tp,
        col,
        gate_proj.reshape(feat, block),
        up_proj.reshape(feat, block),
        down_proj.reshape(block, feat),
        spaces="s",
        outs="h",
        scratch=[pltpu.VMEM((3 * quarter, block), BF16), pltpu.SemaphoreType.DMA],
    )
    packed = [packed[0], *around(packed[1:])]
    both, down = local(
        collect_kernel,
        [half(quarter, 2 * hidden), half(hidden, quarter)],
        col,
        *packed,
        spaces="sh",
        scratch=[pltpu.SemaphoreType.DMA((2 + tp,))],
    )

    far = local(far_kernel, half(some, 3 * hidden), col, got, both, down, spaces="s")
    xg, own, later, *near = local(
        near_kernel,
        [half(slots, 2 * quarter), half(some, 3 * hidden), half(quarter, 2 * hidden)]
        + [half(some, 3 * hidden)] * len(NEAR),
        col,
        got,
        both,
        down,
        spaces="s",
        outs="hhh",
        scratch=[
            pltpu.VMEM((slots, 2 * quarter), BF16),
            pltpu.VMEM((some, 3 * hidden), BF16),
            pltpu.SemaphoreType.DMA((3,)),
        ],
    )
    part = [own, *around([near[0], far, near[1]])]
    grads = local(middle_kernel, half(3 * hidden // LANES * some + PAD, LANES), *part)
    grads = [grads, *around(grads)]

    ready = local(
        ready_kernel,
        half(quarter, 2 * hidden),
        later,
        spaces="h",
        scratch=[pltpu.SemaphoreType.DMA],
    )
    back = local(
        input_kernel,
        half(2 * slots, quarter // 2 + LANES),
        col,
        *grads,
        ready,
        spaces="s",
        outs="h",
        scratch=[
            pltpu.VMEM((2 * slots, quarter // 2 + LANES), BF16),
            pltpu.SemaphoreType.DMA((tp,)),
        ],
    )
    back = over(back, EP)
    one, two, inverse = local(
        pick_kernel,
        [half(slots, rows)] * 2 + [jax.ShapeDtypeStruct((top, rows), F32)],
        routes_t,
        weights_t,
    )
    tokens_grad, weights_grad = local(
        combine_kernel,
        [half(rows, quarter), jax.ShapeDtypeStruct((top, rows), F32)],
        inverse,
        one,
        two,
        back,
    )
    weights_grad = weights_grad.T

    outer = {}
    for steps in ((FAR,), NEAR):
        got = local(
            functools.partial(outer_kernel, steps=steps),
            [half(3 * quarter, block)] * len(steps),
            col,
            xg,
            *grads,
            spaces="s",
        )
        outer.update(zip(steps, got))
    outer = around([outer[k] for k in range(1, tp)])
    whole = [half(feat, block), half(feat, block), half(block, feat)]
    own = local(
        own_kernel,
        whole,
        col,
        xg,
        *grads,
        spaces="s",
        outs="hhh",
        scratch=[
            pltpu.VMEM((quarter, block), BF16),
            pltpu.VMEM((quarter, block), BF16),
            pltpu.VMEM((block, quarter), BF16),
            pltpu.SemaphoreType.DMA((3,)),
        ],
    )
    for steps in ((FAR,), NEAR):
        own = local(
            functools.partial(finish_kernel, steps=steps),
            whole,
            col,
            *[outer[k - 1] for k in steps],
            *own,
            spaces="s" + "v" * len(steps) + "hhh",
            outs="hhh",
            scratch=[pltpu.SemaphoreType.DMA((len(steps) * (2 + tp),))],
            alias={len(steps) + 1 + k: k for k in range(3)},
        )
    gate_grad, up_grad, down_grad = own

    inner = ep // lax.axis_size("z")
    group = feat // ep
    hidden_grad, shared = local(
        dots_kernel,
        [half(rows, block), half(inner, ep // inner, group, block)],
        cotangent,
        shared_hidden,
        shared_down,
    )
    shared = over(shared.reshape(feat, block), ("y", "core"))
    shared = local(
        fold_kernel,
        half(feat // inner, block),
        shared,
        spaces="h",
        scratch=[pltpu.VMEM((feat, block), BF16), pltpu.SemaphoreType.DMA],
    )
    shared = over(shared, "z")
    shared_grad = local(total_kernel, jax.ShapeDtypeStruct((feat // ep, block), F32), shared)
    return (
        tokens_grad,
        weights_grad,
        gate_grad.reshape(gate_proj.shape),
        up_grad.reshape(up_proj.shape),
        down_grad.reshape(down_proj.shape),
        hidden_grad,
        shared_grad,
    )


def solution(mesh):
    devices = mesh.devices
    split = Mesh(devices.reshape(8, -1, 2, devices.shape[-1]), (*EP, "tp"))
    return jax.shard_map(
        experts,
        mesh=split,
        in_specs=(
            P(EP, None),
            P(EP, None),
            P(EP, None),
            P(EP, None),
            P(EP, None, "tp"),
            P(EP, None, "tp"),
            P(EP, "tp", None),
            P(None, "tp"),
            P(EP, "tp"),
        ),
        out_specs=(
            P(EP, "tp"),
            P(EP, None),
            P(EP, None, "tp"),
            P(EP, None, "tp"),
            P(EP, "tp", None),
            P(EP, "tp"),
            P(EP, "tp"),
        ),
        check_vma=False,
    )
```

```python
import functools

import jax
import jax.numpy as jnp
from jax import lax
from jax.experimental import pallas as pl
from jax.experimental.pallas import tpu as pltpu
from jax.sharding import Mesh
from jax.sharding import PartitionSpec as P

EP = ("z", "y", "core")
F32 = jnp.float32
BF16 = jnp.bfloat16
COLS = (((1,), (0,)), ((), ()))
ROWS = (((0,), (0,)), ((), ()))
LAST = (((1,), (1,)), ((), ()))
VMEM = pl.BlockSpec(memory_space=pltpu.VMEM)
SMEM = pl.BlockSpec(memory_space=pltpu.SMEM)
HBM = pl.BlockSpec(memory_space=pltpu.HBM)
LIMIT = pltpu.CompilerParams(vmem_limit_bytes=12 * 2**20)
CAP = 4
CAP_BITS = 2
LANES = 128
PAD = 16
FAR = 2
NEAR = (1, 3)
GROUP = 16


def mm(a, b, dims=COLS):
    return lax.dot_general(a, b, dims, preferred_element_type=F32)


def around(array):
    size = lax.axis_size("tp")
    arrays = array if isinstance(array, (list, tuple)) else [array] * (size - 1)
    got = []
    for k, part in enumerate(arrays):
        got.append(lax.ppermute(part, "tp", [(i, (i + k + 1) % size) for i in range(size)]))
    return got


def over(array, axes):
    size = lax.axis_size(axes)
    rows = array.reshape(size, -1, array.shape[-1])
    return lax.all_to_all(rows, axes, split_axis=0, concat_axis=0, tiled=True).reshape(array.shape)


def at(col, step, parts):
    return lax.rem(col[0] + (step + parts), parts)


def span(index, width):
    return pl.ds(pl.multiple_of(index * width, width), width)


def local(kernel, out, *args, spaces="", outs="", scratch=(), alias=None):
    spec = {"s": SMEM, "v": VMEM, "h": HBM}
    kept = {"h": pltpu.HBM}
    spaces = spaces + "v" * (len(args) - len(spaces))
    args = [
        pltpu.with_memory_space_constraint(a, kept[k]) if k in kept else a
        for a, k in zip(args, spaces)
    ]
    single = not isinstance(out, (list, tuple))
    out = [out] if single else list(out)
    outs = outs + "v" * (len(out) - len(outs))
    out = [kept[k](o.shape, o.dtype) if k in kept else o for o, k in zip(out, outs)]
    got = pl.pallas_call(
        kernel,
        in_specs=[spec[k] for k in spaces],
        out_specs=[spec[k] for k in outs],
        out_shape=out,
        scratch_shapes=scratch,
        input_output_aliases=alias or {},
        compiler_params=LIMIT,
    )(*args)
    return got[0] if single else got


def weave(back=False):
    rows = 64 * CAP
    row = lax.broadcasted_iota(jnp.int32, (rows, rows), int(back))
    col = lax.broadcasted_iota(jnp.int32, (rows, rows), 1 - int(back))
    s, h, r = row >> (CAP_BITS + 1), (row >> CAP_BITS) & 1, row & (CAP - 1)
    place = (h << (CAP_BITS + 5)) + (s << CAP_BITS) + r
    return jnp.where(col == place, 1.0, 0.0).astype(BF16)


def chosen(routes_ref, slots, turns=1, start=0):
    count = routes_ref.shape[1]
    row = start + lax.broadcasted_iota(jnp.int32, (turns * slots, count), 0)
    expert = row >> (CAP_BITS + turns - 1)
    first = expert == routes_ref[0:1, :]
    second = expert == routes_ref[1:2, :]
    named = jnp.where(first | second, 1.0, 0.0)
    earlier = lax.broadcasted_iota(jnp.int32, (count, count), 0)
    later = lax.broadcasted_iota(jnp.int32, (count, count), 1)
    before = jnp.where(earlier < later, 1.0, 0.0).astype(BF16)
    rank = mm(named.astype(BF16), before)
    place = (row & (CAP - 1)).astype(F32)
    hit = jnp.where(rank == place, named, 0.0)
    return hit, jnp.where(first, hit, 0.0), jnp.where(second, hit, 0.0)


def dispatch_kernel(
    col, routes_ref, weights_ref, tok_ref, cot_ref, sent_ref, routes, weights, both, sent, sems
):
    slots = sent_ref.shape[0] // 2
    rows, quarter = tok_ref.shape[0], both.shape[1]
    place = span(col[0], quarter)
    copies = [
        pltpu.make_async_copy(src, dst, sems.at[k])
        for k, (src, dst) in enumerate(
            [
                (routes_ref, routes),
                (weights_ref, weights),
                (tok_ref.at[:, place], both.at[:rows, :]),
                (cot_ref.at[:, place], both.at[rows:, :]),
            ]
        )
    ]
    for copy in copies:
        copy.start()
    half = slots // 2
    leaving = []
    for b in range(2 * slots // half):
        if b == 0:
            copies[0].wait()
        hit, one, two = chosen(routes, half // 2, 2, b * half)
        kind = (lax.broadcasted_iota(jnp.int32, hit.shape, 0) >> CAP_BITS) & 1
        pick = jnp.concatenate(
            [jnp.where(kind == 0, hit, 0.0), jnp.where(kind == 1, hit, 0.0)], axis=1
        )
        if b == 0:
            copies[1].wait()
        scale = weights[...].astype(BF16).astype(F32)
        weight = jnp.sum(one * scale[0:1, :] + two * scale[1:2, :], axis=1, keepdims=True)
        weight = jnp.where(kind[:, 0:1] == 0, 1.0, weight)
        if b == 0:
            copies[2].wait()
            copies[3].wait()
        part = slice(b * half, (b + 1) * half)
        sent[part, :] = (weight * mm(pick.astype(BF16), both[...])).astype(BF16)
        leaving.append(
            pltpu.make_async_copy(sent.at[part, :], sent_ref.at[part, :], sems.at[4 + b])
        )
        leaving[-1].start()
    for copy in leaving:
        copy.wait()


def pick_kernel(routes_ref, weights_ref, one_ref, two_ref, inverse_ref):
    _, one, two = chosen(routes_ref, one_ref.shape[0])
    one_ref[...] = one.astype(BF16)
    two_ref[...] = two.astype(BF16)
    inverse_ref[...] = 1.0 / weights_ref[...].astype(BF16).astype(F32)


def dots_kernel(cot_ref, hid_ref, down_ref, grad_ref, terms_ref):
    cot = cot_ref[...]
    grad_ref[...] = mm(cot, down_ref[...]).astype(BF16)
    terms = mm(cot, hid_ref[...], ROWS).astype(BF16)
    inner, outer, group, width = terms_ref.shape
    terms = terms.reshape(outer, inner, group, width)
    for k in range(outer):
        terms_ref[:, k] = terms[k]


def fold_kernel(terms_ref, out_ref):
    terms = terms_ref[...].astype(F32)
    out_ref[...] = jnp.sum(terms.reshape(-1, *out_ref.shape), axis=0).astype(BF16)


def total_kernel(terms_ref, out_ref):
    rows, width = terms_ref.shape
    terms = terms_ref[...].astype(F32).reshape(rows // GROUP, GROUP, width)
    out_ref[...] = jnp.sum(terms, axis=0)


def pack_kernel(col, gate_ref, up_ref, down_ref, own_out, *refs):
    *outs, own_ref, sem = refs
    parts = len(outs) + 1
    quarter = gate_ref.shape[0] // parts
    block = gate_ref.shape[1]
    own_copy = pltpu.make_async_copy(own_ref, own_out, sem)
    for k, out in enumerate([own_ref, *outs]):
        to = at(col, k, parts)
        out[:quarter, :] = gate_ref[span(to, quarter), :]
        out[quarter : 2 * quarter, :] = up_ref[span(to, quarter), :]
        down = down_ref[:, span(to, quarter)]
        for c in range(quarter // block):
            row = 2 * quarter + c * block
            out[row : row + block, :] = down[:, c * block : (c + 1) * block]
        if k == 0:
            own_copy.start()
    own_copy.wait()


def collect_kernel(col, own_ref, *refs):
    *packed, both_ref, down_ref, sems = refs
    parts = len(packed) + 1
    quarter, width = both_ref.shape
    block = width // (2 * parts)
    copies = []
    for k, ref in enumerate([own_ref, *packed]):
        index = at(col, -k, parts)
        place = span(index, block)
        pairs = [
            (slice(0, quarter), both_ref.at[:, place]),
            (slice(quarter, 2 * quarter), both_ref.at[:, span(index + parts, block)]),
        ]
        for c in range(quarter // block):
            row = 2 * quarter + c * block
            across = slice(c * block, (c + 1) * block)
            pairs.append((slice(row, row + block), down_ref.at[place, across]))
        for rows, out in pairs:
            if k == 0:
                copies.append(pltpu.make_async_copy(ref.at[rows, :], out, sems.at[len(copies)]))
                copies[-1].start()
            else:
                out[...] = ref[rows, :]
    for copy in copies:
        copy.wait()


def apart(order, got):
    split = mm(order, got).astype(BF16)
    half = split.shape[0] // 2
    return split[:half], split[half:]


def far_kernel(col, got_ref, both_ref, down_ref, out_ref):
    rows = out_ref.shape[0]
    parts = got_ref.shape[0] // (2 * rows)
    width = both_ref.shape[1]
    x, g = apart(weave(True), got_ref[span(at(col, FAR, parts), 2 * rows), :])
    out_ref[:, :width] = mm(x, both_ref[...]).astype(BF16)
    out_ref[:, width:] = mm(g, down_ref[...], LAST).astype(BF16)


def near_kernel(col, got_ref, both_ref, down_ref, xg_out, own_out, both_out, *refs):
    *outs, xg_ref, own_ref, sems = refs
    both_copy = pltpu.make_async_copy(both_ref, both_out, sems.at[2])
    both_copy.start()
    rows = own_ref.shape[0]
    parts = got_ref.shape[0] // (2 * rows)
    width = both_ref.shape[1]
    quarter = got_ref.shape[1]
    order = weave(True)
    for b in range(parts):
        x, g = apart(order, got_ref[2 * b * rows : 2 * (b + 1) * rows, :])
        xg_ref[b * rows : (b + 1) * rows, :quarter] = x
        xg_ref[b * rows : (b + 1) * rows, quarter:] = g
    xg_copy = pltpu.make_async_copy(xg_ref, xg_out, sems.at[0])
    xg_copy.start()
    blocks = [span(at(col, k, parts), rows) for k in [0, *NEAR]]
    xg = jnp.concatenate([xg_ref[place, :] for place in blocks], axis=0)
    grown = mm(xg[:, :quarter], both_ref[...]).astype(BF16)
    backed = mm(xg[:, quarter:], down_ref[...], LAST).astype(BF16)
    own_copy = pltpu.make_async_copy(own_ref, own_out, sems.at[1])
    for k, out in enumerate([own_ref, *outs]):
        out[:, :width] = grown[k * rows : (k + 1) * rows]
        out[:, width:] = backed[k * rows : (k + 1) * rows]
        if k == 0:
            own_copy.start()
    xg_copy.wait()
    own_copy.wait()
    both_copy.wait()


def diagonal(size):
    row = lax.broadcasted_iota(jnp.int32, (size, size), 0)
    return row == lax.broadcasted_iota(jnp.int32, (size, size), 1)


def middle_kernel(*refs):
    *parts, grads_ref = refs
    rows, width = parts[0].shape
    hidden = width // 3
    total = parts[0][...].astype(F32)
    for ref in parts[1:]:
        total = total + ref[...].astype(F32)
    gate = total[:, :hidden]
    upper = total[:, hidden : 2 * hidden]
    backed = total[:, 2 * hidden :]
    sigma = jax.nn.sigmoid(gate)
    active = gate * sigma
    hid = (active * upper).astype(BF16)
    d_gate = (backed * upper * sigma * (1.0 + gate * (1.0 - sigma))).astype(BF16)
    d_up = (backed * active).astype(BF16)
    blocks = hidden // LANES
    for k, value in enumerate([d_gate, d_up, hid]):
        for c in range(blocks):
            row = (k * blocks + c) * rows
            grads_ref[row : row + rows, :] = value[:, c * LANES : (c + 1) * LANES]
    share = jnp.sum(hid.astype(F32) * backed, axis=1, keepdims=True)
    share = jnp.sum(jnp.where(diagonal(rows), share, 0.0), axis=0, keepdims=True)
    grads_ref[3 * blocks * rows :, :] = jnp.broadcast_to(share, (PAD, LANES)).astype(BF16)


def ready_kernel(both_hbm, both_ref, sem):
    copy = pltpu.make_async_copy(both_hbm, both_ref, sem)
    copy.start()
    copy.wait()


def input_kernel(col, *refs):
    *grads, both_ref, back_out, out_ref, sems = refs
    parts = len(grads)
    rows = out_ref.shape[0] // (2 * parts)
    blocks = both_ref.shape[1] // LANES
    whole = jnp.concatenate(
        [
            jnp.concatenate([ref[c * rows : (c + 1) * rows, :] for c in range(blocks)], axis=1)
            for ref in grads
        ],
        axis=0,
    )
    out = mm(whole, both_ref[...], LAST).astype(BF16)
    order = weave()
    half = out.shape[1] // 2
    copies = []
    for k, ref in enumerate(grads):
        own = out[k * rows : (k + 1) * rows]
        both = jnp.concatenate([own[:, :half], own[:, half:]], axis=0)
        place = slice(2 * k * rows, 2 * (k + 1) * rows)
        out_ref[place, :half] = mm(order, both).astype(BF16)
        share = ref[ref.shape[0] - PAD :, :].astype(F32)[0:1]
        share = jnp.sum(jnp.where(diagonal(rows), share, 0.0), axis=1, keepdims=True)
        share = jnp.broadcast_to(share, (rows, LANES)).astype(BF16)
        out_ref[place, half:] = mm(order[:, :rows], share).astype(BF16)
        to = back_out.at[span(at(col, -k, parts), 2 * rows), :]
        copies.append(pltpu.make_async_copy(out_ref.at[place, :], to, sems.at[k]))
        copies[-1].start()
    for copy in copies:
        copy.wait()


def outer_terms(col, steps, xg_ref, grads):
    parts = len(grads)
    rows = xg_ref.shape[0] // parts
    block = LANES
    quarter = xg_ref.shape[1] // 2
    order = [span(at(col, -k, parts), rows) for k in range(parts)]
    x = jnp.concatenate([xg_ref[place, :quarter] for place in order], axis=0)
    g = jnp.concatenate([xg_ref[place, quarter:] for place in order], axis=0)

    def units(kinds):
        places = [span(at(col, k, parts) + kind * parts, rows) for k in steps for kind in kinds]
        return jnp.concatenate(
            [jnp.concatenate([ref[place, :] for place in places], axis=1) for ref in grads], axis=0
        )

    both = mm(x, units((0, 1)), ROWS).astype(BF16)
    down = mm(units((2,)), g, ROWS).astype(BF16)
    return [
        (
            both[:, 2 * n * block : (2 * n + 1) * block],
            both[:, (2 * n + 1) * block : (2 * n + 2) * block],
            down[n * block : (n + 1) * block],
        )
        for n in range(len(steps))
    ]


def outer_kernel(col, xg_ref, *refs, steps):
    grads, outs = refs[: -len(steps)], refs[-len(steps) :]
    for out, (gate, up, down) in zip(outs, outer_terms(col, steps, xg_ref, grads)):
        quarter, block = gate.shape
        out[:quarter, :] = gate
        out[quarter : 2 * quarter, :] = up
        for c in range(quarter // block):
            row = 2 * quarter + c * block
            out[row : row + block, :] = down[:, c * block : (c + 1) * block]


def own_kernel(col, xg_ref, *refs):
    *grads, gate_out, up_out, down_out, gate_ref, up_ref, down_ref, sems = refs
    place = span(at(col, 0, len(grads)), gate_ref.shape[0])
    [(gate, up, down)] = outer_terms(col, (0,), xg_ref, grads)
    gate_ref[...] = gate
    up_ref[...] = up
    down_ref[...] = down
    copies = [
        pltpu.make_async_copy(gate_ref, gate_out.at[place, :], sems.at[0]),
        pltpu.make_async_copy(up_ref, up_out.at[place, :], sems.at[1]),
        pltpu.make_async_copy(down_ref, down_out.at[:, place], sems.at[2]),
    ]
    for copy in copies:
        copy.start()
    for copy in copies:
        copy.wait()


def finish_kernel(col, *refs, steps):
    *refs, sems = refs
    got, (gate_ref, up_ref, down_ref) = refs[: len(steps)], refs[-3:]
    block = gate_ref.shape[1]
    quarter = got[0].shape[0] // 3
    parts = gate_ref.shape[0] // quarter
    copies = []
    for k, ref in zip(steps, got):
        index = at(col, -k, parts)
        place = span(index, quarter)
        pairs = [
            (ref.at[:quarter, :], gate_ref.at[place, :]),
            (ref.at[quarter : 2 * quarter, :], up_ref.at[place, :]),
        ]
        for c in range(quarter // block):
            row = 2 * quarter + c * block
            across = span(index * (quarter // block) + c, block)
            pairs.append((ref.at[row : row + block, :], down_ref.at[:, across]))
        for src, dst in pairs:
            copies.append(pltpu.make_async_copy(src, dst, sems.at[len(copies)]))
            copies[-1].start()
    for copy in copies:
        copy.wait()


def combine_kernel(inverse_ref, one_ref, two_ref, back_ref, out_ref, weights_out):
    slots = one_ref.shape[0]
    order = weave(True)
    half = order.shape[0] // 2
    width = out_ref.shape[1] // 2
    left, right, shares = [], [], []
    for b in range(slots // half):
        own = mm(order, back_ref[2 * b * half : 2 * (b + 1) * half, :]).astype(BF16)
        left.append(own[:half, :width])
        right.append(own[half:, :width])
        shares.append(own[:half, width:].astype(F32))
    one = one_ref[...]
    two = two_ref[...]
    pick = one + two
    out_ref[:, :width] = mm(pick, jnp.concatenate(left, axis=0), ROWS).astype(BF16)
    out_ref[:, width:] = mm(pick, jnp.concatenate(right, axis=0), ROWS).astype(BF16)
    share = jnp.concatenate(shares, axis=0)
    for k, mask in enumerate([one, two]):
        total = jnp.sum(mask.astype(F32) * share, axis=0, keepdims=True)
        weights_out[k : k + 1, :] = total * inverse_ref[k : k + 1, :]


def experts(
    tokens,
    cotangent,
    route_weights,
    routes,
    gate_proj,
    up_proj,
    down_proj,
    shared_down,
    shared_hidden,
):
    rows, feat = tokens.shape
    top = routes.shape[1]
    ep = lax.axis_size(EP)
    tp = lax.axis_size("tp")
    slots = ep * CAP
    quarter = feat // tp
    block = gate_proj.shape[2]
    hidden = block * tp
    some = slots // tp
    half = lambda *shape: jax.ShapeDtypeStruct(shape, BF16)
    col = lax.axis_index("tp").astype(jnp.int32).reshape(1)
    routes_t = routes.T
    weights_t = route_weights.T

    sent = local(
        dispatch_kernel,
        half(2 * slots, quarter),
        col,
        routes_t,
        weights_t,
        tokens,
        cotangent,
        spaces="shhhh",
        outs="h",
        scratch=[
            pltpu.VMEM(routes_t.shape, jnp.int32),
            pltpu.VMEM(weights_t.shape, F32),
            pltpu.VMEM((2 * rows, quarter), BF16),
            pltpu.VMEM((2 * slots, quarter), BF16),
            pltpu.SemaphoreType.DMA((4 + tp,)),
        ],
    )
    got = over(sent, EP)

    packed = local(
        pack_kernel,
        [half(3 * quarter, block)] * tp,
        col,
        gate_proj.reshape(feat, block),
        up_proj.reshape(feat, block),
        down_proj.reshape(block, feat),
        spaces="s",
        outs="h",
        scratch=[pltpu.VMEM((3 * quarter, block), BF16), pltpu.SemaphoreType.DMA],
    )
    packed = [packed[0], *around(packed[1:])]
    both, down = local(
        collect_kernel,
        [half(quarter, 2 * hidden), half(hidden, quarter)],
        col,
        *packed,
        spaces="sh",
        scratch=[pltpu.SemaphoreType.DMA((2 + tp,))],
    )

    far = local(far_kernel, half(some, 3 * hidden), col, got, both, down, spaces="s")
    xg, own, later, *near = local(
        near_kernel,
        [half(slots, 2 * quarter), half(some, 3 * hidden), half(quarter, 2 * hidden)]
        + [half(some, 3 * hidden)] * len(NEAR),
        col,
        got,
        both,
        down,
        spaces="s",
        outs="hhh",
        scratch=[
            pltpu.VMEM((slots, 2 * quarter), BF16),
            pltpu.VMEM((some, 3 * hidden), BF16),
            pltpu.SemaphoreType.DMA((3,)),
        ],
    )
    part = [own, *around([near[0], far, near[1]])]
    grads = local(middle_kernel, half(3 * hidden // LANES * some + PAD, LANES), *part)
    grads = [grads, *around(grads)]

    ready = local(
        ready_kernel,
        half(quarter, 2 * hidden),
        later,
        spaces="h",
        scratch=[pltpu.SemaphoreType.DMA],
    )
    back = local(
        input_kernel,
        half(2 * slots, quarter // 2 + LANES),
        col,
        *grads,
        ready,
        spaces="s",
        outs="h",
        scratch=[
            pltpu.VMEM((2 * slots, quarter // 2 + LANES), BF16),
            pltpu.SemaphoreType.DMA((tp,)),
        ],
    )
    back = over(back, EP)
    one, two, inverse = local(
        pick_kernel,
        [half(slots, rows)] * 2 + [jax.ShapeDtypeStruct((top, rows), F32)],
        routes_t,
        weights_t,
    )
    tokens_grad, weights_grad = local(
        combine_kernel,
        [half(rows, quarter), jax.ShapeDtypeStruct((top, rows), F32)],
        inverse,
        one,
        two,
        back,
    )
    weights_grad = weights_grad.T

    outer = {}
    for steps in ((FAR,), NEAR):
        got = local(
            functools.partial(outer_kernel, steps=steps),
            [half(3 * quarter, block)] * len(steps),
            col,
            xg,
            *grads,
            spaces="s",
        )
        outer.update(zip(steps, got))
    outer = around([outer[k] for k in range(1, tp)])
    whole = [half(feat, block), half(feat, block), half(block, feat)]
    own = local(
        own_kernel,
        whole,
        col,
        xg,
        *grads,
        spaces="s",
        outs="hhh",
        scratch=[
            pltpu.VMEM((quarter, block), BF16),
            pltpu.VMEM((quarter, block), BF16),
            pltpu.VMEM((block, quarter), BF16),
            pltpu.SemaphoreType.DMA((3,)),
        ],
    )
    for steps in ((FAR,), NEAR):
        own = local(
            functools.partial(finish_kernel, steps=steps),
            whole,
            col,
            *[outer[k - 1] for k in steps],
            *own,
            spaces="s" + "v" * len(steps) + "hhh",
            outs="hhh",
            scratch=[pltpu.SemaphoreType.DMA((len(steps) * (2 + tp),))],
            alias={len(steps) + 1 + k: k for k in range(3)},
        )
    gate_grad, up_grad, down_grad = own

    inner = ep // lax.axis_size("z")
    group = feat // ep
    hidden_grad, shared = local(
        dots_kernel,
        [half(rows, block), half(inner, ep // inner, group, block)],
        cotangent,
        shared_hidden,
        shared_down,
    )
    shared = over(shared.reshape(feat, block), ("y", "core"))
    shared = local(fold_kernel, half(feat // inner, block), shared)
    shared = over(shared, "z")
    shared_grad = local(
        total_kernel, jax.ShapeDtypeStruct((feat // ep, block), F32), shared
    )
    return (
        tokens_grad,
        weights_grad,
        gate_grad.reshape(gate_proj.shape),
        up_grad.reshape(up_proj.shape),
        down_grad.reshape(down_proj.shape),
        hidden_grad,
        shared_grad,
    )


def solution(mesh):
    devices = mesh.devices
    split = Mesh(devices.reshape(8, -1, 2, devices.shape[-1]), (*EP, "tp"))
    return jax.shard_map(
        experts,
        mesh=split,
        in_specs=(
            P(EP, None),
            P(EP, None),
            P(EP, None),
            P(EP, None),
            P(EP, None, "tp"),
            P(EP, None, "tp"),
            P(EP, "tp", None),
            P(None, "tp"),
            P(EP, "tp"),
        ),
        out_specs=(
            P(EP, "tp"),
            P(EP, None),
            P(EP, None, "tp"),
            P(EP, None, "tp"),
            P(EP, "tp", None),
            P(EP, "tp"),
            P(EP, "tp"),
        ),
        check_vma=False,
    )
```

```python
import functools

import jax
import jax.numpy as jnp
from jax import lax
from jax.experimental import pallas as pl
from jax.experimental.pallas import tpu as pltpu
from jax.sharding import Mesh
from jax.sharding import PartitionSpec as P

EP = ("z", "y", "core")
F32 = jnp.float32
BF16 = jnp.bfloat16
COLS = (((1,), (0,)), ((), ()))
ROWS = (((0,), (0,)), ((), ()))
LAST = (((1,), (1,)), ((), ()))
VMEM = pl.BlockSpec(memory_space=pltpu.VMEM)
SMEM = pl.BlockSpec(memory_space=pltpu.SMEM)
HBM = pl.BlockSpec(memory_space=pltpu.HBM)
LIMIT = pltpu.CompilerParams(vmem_limit_bytes=12 * 2**20)
CAP = 4
CAP_BITS = 2
LANES = 128
PAD = 16
FAR = 2
NEAR = (1, 3)
GROUP = 16


def mm(a, b, dims=COLS):
    return lax.dot_general(a, b, dims, preferred_element_type=F32)


def around(array):
    size = lax.axis_size("tp")
    arrays = array if isinstance(array, (list, tuple)) else [array] * (size - 1)
    got = []
    for k, part in enumerate(arrays):
        got.append(lax.ppermute(part, "tp", [(i, (i + k + 1) % size) for i in range(size)]))
    return got


def over(array, axes):
    size = lax.axis_size(axes)
    rows = array.reshape(size, -1, array.shape[-1])
    return lax.all_to_all(rows, axes, split_axis=0, concat_axis=0, tiled=True).reshape(array.shape)


def at(col, step, parts):
    return lax.rem(col[0] + (step + parts), parts)


def span(index, width):
    return pl.ds(pl.multiple_of(index * width, width), width)


def local(kernel, out, *args, spaces="", outs="", scratch=(), alias=None):
    spec = {"s": SMEM, "v": VMEM, "h": HBM}
    kept = {"h": pltpu.HBM}
    spaces = spaces + "v" * (len(args) - len(spaces))
    args = [
        pltpu.with_memory_space_constraint(a, kept[k]) if k in kept else a
        for a, k in zip(args, spaces)
    ]
    single = not isinstance(out, (list, tuple))
    out = [out] if single else list(out)
    outs = outs + "v" * (len(out) - len(outs))
    out = [kept[k](o.shape, o.dtype) if k in kept else o for o, k in zip(out, outs)]
    got = pl.pallas_call(
        kernel,
        in_specs=[spec[k] for k in spaces],
        out_specs=[spec[k] for k in outs],
        out_shape=out,
        scratch_shapes=scratch,
        input_output_aliases=alias or {},
        compiler_params=LIMIT,
    )(*args)
    return got[0] if single else got


def weave(back=False):
    rows = 64 * CAP
    row = lax.broadcasted_iota(jnp.int32, (rows, rows), int(back))
    col = lax.broadcasted_iota(jnp.int32, (rows, rows), 1 - int(back))
    s, h, r = row >> (CAP_BITS + 1), (row >> CAP_BITS) & 1, row & (CAP - 1)
    place = (h << (CAP_BITS + 5)) + (s << CAP_BITS) + r
    return jnp.where(col == place, 1.0, 0.0).astype(BF16)


def chosen(routes_ref, slots, turns=1, start=0):
    count = routes_ref.shape[1]
    row = start + lax.broadcasted_iota(jnp.int32, (turns * slots, count), 0)
    expert = row >> (CAP_BITS + turns - 1)
    first = expert == routes_ref[0:1, :]
    second = expert == routes_ref[1:2, :]
    named = jnp.where(first | second, 1.0, 0.0)
    earlier = lax.broadcasted_iota(jnp.int32, (count, count), 0)
    later = lax.broadcasted_iota(jnp.int32, (count, count), 1)
    before = jnp.where(earlier < later, 1.0, 0.0).astype(BF16)
    rank = mm(named.astype(BF16), before)
    place = (row & (CAP - 1)).astype(F32)
    hit = jnp.where(rank == place, named, 0.0)
    return hit, jnp.where(first, hit, 0.0), jnp.where(second, hit, 0.0)


def dispatch_kernel(
    col, routes_ref, weights_ref, tok_ref, cot_ref, sent_ref, routes, weights, both, sent, sems
):
    slots = sent_ref.shape[0] // 2
    rows, quarter = tok_ref.shape[0], both.shape[1]
    place = span(col[0], quarter)
    copies = [
        pltpu.make_async_copy(src, dst, sems.at[k])
        for k, (src, dst) in enumerate(
            [
                (routes_ref, routes),
                (weights_ref, weights),
                (tok_ref.at[:, place], both.at[:rows, :]),
                (cot_ref.at[:, place], both.at[rows:, :]),
            ]
        )
    ]
    for copy in copies:
        copy.start()
    half = slots // 2
    leaving = []
    for b in range(2 * slots // half):
        if b == 0:
            copies[0].wait()
        hit, one, two = chosen(routes, half // 2, 2, b * half)
        kind = (lax.broadcasted_iota(jnp.int32, hit.shape, 0) >> CAP_BITS) & 1
        pick = jnp.concatenate(
            [jnp.where(kind == 0, hit, 0.0), jnp.where(kind == 1, hit, 0.0)], axis=1
        )
        if b == 0:
            copies[1].wait()
        scale = weights[...].astype(BF16).astype(F32)
        weight = jnp.sum(one * scale[0:1, :] + two * scale[1:2, :], axis=1, keepdims=True)
        weight = jnp.where(kind[:, 0:1] == 0, 1.0, weight)
        if b == 0:
            copies[2].wait()
            copies[3].wait()
        part = slice(b * half, (b + 1) * half)
        sent[part, :] = (weight * mm(pick.astype(BF16), both[...])).astype(BF16)
        leaving.append(
            pltpu.make_async_copy(sent.at[part, :], sent_ref.at[part, :], sems.at[4 + b])
        )
        leaving[-1].start()
    for copy in leaving:
        copy.wait()


def pick_kernel(routes_ref, weights_ref, one_ref, two_ref, inverse_ref):
    _, one, two = chosen(routes_ref, one_ref.shape[0])
    one_ref[...] = one.astype(BF16)
    two_ref[...] = two.astype(BF16)
    inverse_ref[...] = 1.0 / weights_ref[...].astype(BF16).astype(F32)


def dots_kernel(cot_ref, hid_ref, down_ref, grad_ref, terms_ref):
    cot = cot_ref[...]
    grad_ref[...] = mm(cot, down_ref[...]).astype(BF16)
    terms = mm(cot, hid_ref[...], ROWS).astype(BF16)
    inner, outer, group, width = terms_ref.shape
    terms = terms.reshape(outer, inner, group, width)
    for k in range(outer):
        terms_ref[:, k] = terms[k]


def fold_kernel(terms_ref, out_ref):
    terms = terms_ref[...].astype(F32)
    out_ref[...] = jnp.sum(terms.reshape(-1, *out_ref.shape), axis=0).astype(BF16)


def total_kernel(terms_ref, out_ref):
    rows, width = terms_ref.shape
    terms = terms_ref[...].astype(F32).reshape(rows // GROUP, GROUP, width)
    out_ref[...] = jnp.sum(terms, axis=0)


def pack_kernel(col, gate_ref, up_ref, down_ref, own_out, *refs):
    *outs, own_ref, sem = refs
    parts = len(outs) + 1
    quarter = gate_ref.shape[0] // parts
    block = gate_ref.shape[1]
    own_copy = pltpu.make_async_copy(own_ref, own_out, sem)
    for k, out in enumerate([own_ref, *outs]):
        to = at(col, k, parts)
        out[:quarter, :] = gate_ref[span(to, quarter), :]
        out[quarter : 2 * quarter, :] = up_ref[span(to, quarter), :]
        down = down_ref[:, span(to, quarter)]
        for c in range(quarter // block):
            row = 2 * quarter + c * block
            out[row : row + block, :] = down[:, c * block : (c + 1) * block]
        if k == 0:
            own_copy.start()
    own_copy.wait()


def collect_kernel(col, own_ref, *refs):
    *packed, both_ref, down_ref, sems = refs
    parts = len(packed) + 1
    quarter, width = both_ref.shape
    block = width // (2 * parts)
    copies = []
    for k, ref in enumerate([own_ref, *packed]):
        index = at(col, -k, parts)
        place = span(index, block)
        pairs = [
            (slice(0, quarter), both_ref.at[:, place]),
            (slice(quarter, 2 * quarter), both_ref.at[:, span(index + parts, block)]),
        ]
        for c in range(quarter // block):
            row = 2 * quarter + c * block
            across = slice(c * block, (c + 1) * block)
            pairs.append((slice(row, row + block), down_ref.at[place, across]))
        for rows, out in pairs:
            if k == 0:
                copies.append(pltpu.make_async_copy(ref.at[rows, :], out, sems.at[len(copies)]))
                copies[-1].start()
            else:
                out[...] = ref[rows, :]
    for copy in copies:
        copy.wait()


def apart(order, got):
    split = mm(order, got).astype(BF16)
    half = split.shape[0] // 2
    return split[:half], split[half:]


def far_kernel(col, got_ref, both_ref, down_ref, out_ref):
    rows = out_ref.shape[0]
    parts = got_ref.shape[0] // (2 * rows)
    width = both_ref.shape[1]
    x, g = apart(weave(True), got_ref[span(at(col, FAR, parts), 2 * rows), :])
    out_ref[:, :width] = mm(x, both_ref[...]).astype(BF16)
    out_ref[:, width:] = mm(g, down_ref[...], LAST).astype(BF16)


def near_kernel(col, got_ref, both_ref, down_ref, xg_out, own_out, both_out, *refs):
    *outs, xg_ref, own_ref, sems = refs
    both_copy = pltpu.make_async_copy(both_ref, both_out, sems.at[2])
    both_copy.start()
    rows = own_ref.shape[0]
    parts = got_ref.shape[0] // (2 * rows)
    width = both_ref.shape[1]
    quarter = got_ref.shape[1]
    order = weave(True)
    for b in range(parts):
        x, g = apart(order, got_ref[2 * b * rows : 2 * (b + 1) * rows, :])
        xg_ref[b * rows : (b + 1) * rows, :quarter] = x
        xg_ref[b * rows : (b + 1) * rows, quarter:] = g
    xg_copy = pltpu.make_async_copy(xg_ref, xg_out, sems.at[0])
    xg_copy.start()
    blocks = [span(at(col, k, parts), rows) for k in [0, *NEAR]]
    xg = jnp.concatenate([xg_ref[place, :] for place in blocks], axis=0)
    grown = mm(xg[:, :quarter], both_ref[...]).astype(BF16)
    backed = mm(xg[:, quarter:], down_ref[...], LAST).astype(BF16)
    own_copy = pltpu.make_async_copy(own_ref, own_out, sems.at[1])
    for k, out in enumerate([own_ref, *outs]):
        out[:, :width] = grown[k * rows : (k + 1) * rows]
        out[:, width:] = backed[k * rows : (k + 1) * rows]
        if k == 0:
            own_copy.start()
    xg_copy.wait()
    own_copy.wait()
    both_copy.wait()


def diagonal(size):
    row = lax.broadcasted_iota(jnp.int32, (size, size), 0)
    return row == lax.broadcasted_iota(jnp.int32, (size, size), 1)


def middle_kernel(*refs):
    *parts, grads_ref = refs
    rows, width = parts[0].shape
    hidden = width // 3
    total = parts[0][...].astype(F32)
    for ref in parts[1:]:
        total = total + ref[...].astype(F32)
    gate = total[:, :hidden]
    upper = total[:, hidden : 2 * hidden]
    backed = total[:, 2 * hidden :]
    sigma = jax.nn.sigmoid(gate)
    active = gate * sigma
    hid = (active * upper).astype(BF16)
    d_gate = (backed * upper * sigma * (1.0 + gate * (1.0 - sigma))).astype(BF16)
    d_up = (backed * active).astype(BF16)
    blocks = hidden // LANES
    for k, value in enumerate([d_gate, d_up, hid]):
        for c in range(blocks):
            row = (k * blocks + c) * rows
            grads_ref[row : row + rows, :] = value[:, c * LANES : (c + 1) * LANES]
    share = jnp.sum(hid.astype(F32) * backed, axis=1, keepdims=True)
    share = jnp.sum(jnp.where(diagonal(rows), share, 0.0), axis=0, keepdims=True)
    grads_ref[3 * blocks * rows :, :] = jnp.broadcast_to(share, (PAD, LANES)).astype(BF16)


def ready_kernel(both_hbm, both_ref, sem):
    copy = pltpu.make_async_copy(both_hbm, both_ref, sem)
    copy.start()
    copy.wait()


def input_kernel(col, *refs):
    *grads, both_ref, back_out, out_ref, sems = refs
    parts = len(grads)
    rows = out_ref.shape[0] // (2 * parts)
    blocks = both_ref.shape[1] // LANES
    order = weave()
    half = both_ref.shape[0] // 2
    copies = []
    for first in range(0, parts, 2):
        pair = grads[first : first + 2]
        whole = jnp.concatenate(
            [
                jnp.concatenate([ref[c * rows : (c + 1) * rows, :] for c in range(blocks)], axis=1)
                for ref in pair
            ],
            axis=0,
        )
        out = mm(whole, both_ref[...], LAST).astype(BF16)
        for n, ref in enumerate(pair):
            k = first + n
            own = out[n * rows : (n + 1) * rows]
            both = jnp.concatenate([own[:, :half], own[:, half:]], axis=0)
            place = slice(2 * k * rows, 2 * (k + 1) * rows)
            out_ref[place, :half] = mm(order, both).astype(BF16)
            share = ref[ref.shape[0] - PAD :, :].astype(F32)[0:1]
            share = jnp.sum(jnp.where(diagonal(rows), share, 0.0), axis=1, keepdims=True)
            share = jnp.broadcast_to(share, (rows, LANES)).astype(BF16)
            out_ref[place, half:] = mm(order[:, :rows], share).astype(BF16)
            to = back_out.at[span(at(col, -k, parts), 2 * rows), :]
            copies.append(pltpu.make_async_copy(out_ref.at[place, :], to, sems.at[k]))
            copies[-1].start()
    for copy in copies:
        copy.wait()


def outer_terms(col, steps, xg_ref, grads):
    parts = len(grads)
    rows = xg_ref.shape[0] // parts
    block = LANES
    quarter = xg_ref.shape[1] // 2
    order = [span(at(col, -k, parts), rows) for k in range(parts)]
    x = jnp.concatenate([xg_ref[place, :quarter] for place in order], axis=0)
    g = jnp.concatenate([xg_ref[place, quarter:] for place in order], axis=0)

    def units(kinds):
        places = [span(at(col, k, parts) + kind * parts, rows) for k in steps for kind in kinds]
        return jnp.concatenate(
            [jnp.concatenate([ref[place, :] for place in places], axis=1) for ref in grads], axis=0
        )

    both = mm(x, units((0, 1)), ROWS).astype(BF16)
    down = mm(units((2,)), g, ROWS).astype(BF16)
    return [
        (
            both[:, 2 * n * block : (2 * n + 1) * block],
            both[:, (2 * n + 1) * block : (2 * n + 2) * block],
            down[n * block : (n + 1) * block],
        )
        for n in range(len(steps))
    ]


def outer_kernel(col, xg_ref, *refs, steps):
    grads, outs = refs[: -len(steps)], refs[-len(steps) :]
    for out, (gate, up, down) in zip(outs, outer_terms(col, steps, xg_ref, grads)):
        quarter, block = gate.shape
        out[:quarter, :] = gate
        out[quarter : 2 * quarter, :] = up
        for c in range(quarter // block):
            row = 2 * quarter + c * block
            out[row : row + block, :] = down[:, c * block : (c + 1) * block]


def own_kernel(col, xg_ref, *refs):
    *grads, gate_out, up_out, down_out, gate_ref, up_ref, down_ref, sems = refs
    place = span(at(col, 0, len(grads)), gate_ref.shape[0])
    [(gate, up, down)] = outer_terms(col, (0,), xg_ref, grads)
    gate_ref[...] = gate
    up_ref[...] = up
    down_ref[...] = down
    copies = [
        pltpu.make_async_copy(gate_ref, gate_out.at[place, :], sems.at[0]),
        pltpu.make_async_copy(up_ref, up_out.at[place, :], sems.at[1]),
        pltpu.make_async_copy(down_ref, down_out.at[:, place], sems.at[2]),
    ]
    for copy in copies:
        copy.start()
    for copy in copies:
        copy.wait()


def finish_kernel(col, *refs, steps):
    *refs, sems = refs
    got, (gate_ref, up_ref, down_ref) = refs[: len(steps)], refs[-3:]
    block = gate_ref.shape[1]
    quarter = got[0].shape[0] // 3
    parts = gate_ref.shape[0] // quarter
    copies = []
    for k, ref in zip(steps, got):
        index = at(col, -k, parts)
        place = span(index, quarter)
        pairs = [
            (ref.at[:quarter, :], gate_ref.at[place, :]),
            (ref.at[quarter : 2 * quarter, :], up_ref.at[place, :]),
        ]
        for c in range(quarter // block):
            row = 2 * quarter + c * block
            across = span(index * (quarter // block) + c, block)
            pairs.append((ref.at[row : row + block, :], down_ref.at[:, across]))
        for src, dst in pairs:
            copies.append(pltpu.make_async_copy(src, dst, sems.at[len(copies)]))
            copies[-1].start()
    for copy in copies:
        copy.wait()


def combine_kernel(inverse_ref, one_ref, two_ref, back_ref, out_ref, weights_out):
    slots = one_ref.shape[0]
    order = weave(True)
    half = order.shape[0] // 2
    width = out_ref.shape[1] // 2
    left, right, shares = [], [], []
    for b in range(slots // half):
        own = mm(order, back_ref[2 * b * half : 2 * (b + 1) * half, :]).astype(BF16)
        left.append(own[:half, :width])
        right.append(own[half:, :width])
        shares.append(own[:half, width:].astype(F32))
    one = one_ref[...]
    two = two_ref[...]
    pick = one + two
    out_ref[:, :width] = mm(pick, jnp.concatenate(left, axis=0), ROWS).astype(BF16)
    out_ref[:, width:] = mm(pick, jnp.concatenate(right, axis=0), ROWS).astype(BF16)
    share = jnp.concatenate(shares, axis=0)
    for k, mask in enumerate([one, two]):
        total = jnp.sum(mask.astype(F32) * share, axis=0, keepdims=True)
        weights_out[k : k + 1, :] = total * inverse_ref[k : k + 1, :]


def experts(
    tokens,
    cotangent,
    route_weights,
    routes,
    gate_proj,
    up_proj,
    down_proj,
    shared_down,
    shared_hidden,
):
    rows, feat = tokens.shape
    top = routes.shape[1]
    ep = lax.axis_size(EP)
    tp = lax.axis_size("tp")
    slots = ep * CAP
    quarter = feat // tp
    block = gate_proj.shape[2]
    hidden = block * tp
    some = slots // tp
    half = lambda *shape: jax.ShapeDtypeStruct(shape, BF16)
    col = lax.axis_index("tp").astype(jnp.int32).reshape(1)
    routes_t = routes.T
    weights_t = route_weights.T

    sent = local(
        dispatch_kernel,
        half(2 * slots, quarter),
        col,
        routes_t,
        weights_t,
        tokens,
        cotangent,
        spaces="shhhh",
        outs="h",
        scratch=[
            pltpu.VMEM(routes_t.shape, jnp.int32),
            pltpu.VMEM(weights_t.shape, F32),
            pltpu.VMEM((2 * rows, quarter), BF16),
            pltpu.VMEM((2 * slots, quarter), BF16),
            pltpu.SemaphoreType.DMA((4 + tp,)),
        ],
    )
    got = over(sent, EP)

    packed = local(
        pack_kernel,
        [half(3 * quarter, block)] * tp,
        col,
        gate_proj.reshape(feat, block),
        up_proj.reshape(feat, block),
        down_proj.reshape(block, feat),
        spaces="s",
        outs="h",
        scratch=[pltpu.VMEM((3 * quarter, block), BF16), pltpu.SemaphoreType.DMA],
    )
    packed = [packed[0], *around(packed[1:])]
    both, down = local(
        collect_kernel,
        [half(quarter, 2 * hidden), half(hidden, quarter)],
        col,
        *packed,
        spaces="sh",
        scratch=[pltpu.SemaphoreType.DMA((2 + tp,))],
    )

    far = local(far_kernel, half(some, 3 * hidden), col, got, both, down, spaces="s")
    xg, own, later, *near = local(
        near_kernel,
        [half(slots, 2 * quarter), half(some, 3 * hidden), half(quarter, 2 * hidden)]
        + [half(some, 3 * hidden)] * len(NEAR),
        col,
        got,
        both,
        down,
        spaces="s",
        outs="hhh",
        scratch=[
            pltpu.VMEM((slots, 2 * quarter), BF16),
            pltpu.VMEM((some, 3 * hidden), BF16),
            pltpu.SemaphoreType.DMA((3,)),
        ],
    )
    part = [own, *around([near[0], far, near[1]])]
    grads = local(middle_kernel, half(3 * hidden // LANES * some + PAD, LANES), *part)
    grads = [grads, *around(grads)]

    ready = local(
        ready_kernel,
        half(quarter, 2 * hidden),
        later,
        spaces="h",
        scratch=[pltpu.SemaphoreType.DMA],
    )
    back = local(
        input_kernel,
        half(2 * slots, quarter // 2 + LANES),
        col,
        *grads,
        ready,
        spaces="s",
        outs="h",
        scratch=[
            pltpu.VMEM((2 * slots, quarter // 2 + LANES), BF16),
            pltpu.SemaphoreType.DMA((tp,)),
        ],
    )
    back = over(back, EP)
    one, two, inverse = local(
        pick_kernel,
        [half(slots, rows)] * 2 + [jax.ShapeDtypeStruct((top, rows), F32)],
        routes_t,
        weights_t,
    )
    tokens_grad, weights_grad = local(
        combine_kernel,
        [half(rows, quarter), jax.ShapeDtypeStruct((top, rows), F32)],
        inverse,
        one,
        two,
        back,
    )
    weights_grad = weights_grad.T

    outer = {}
    for steps in ((FAR,), NEAR):
        got = local(
            functools.partial(outer_kernel, steps=steps),
            [half(3 * quarter, block)] * len(steps),
            col,
            xg,
            *grads,
            spaces="s",
        )
        outer.update(zip(steps, got))
    outer = around([outer[k] for k in range(1, tp)])
    whole = [half(feat, block), half(feat, block), half(block, feat)]
    own = local(
        own_kernel,
        whole,
        col,
        xg,
        *grads,
        spaces="s",
        outs="hhh",
        scratch=[
            pltpu.VMEM((quarter, block), BF16),
            pltpu.VMEM((quarter, block), BF16),
            pltpu.VMEM((block, quarter), BF16),
            pltpu.SemaphoreType.DMA((3,)),
        ],
    )
    for steps in ((FAR,), NEAR):
        own = local(
            functools.partial(finish_kernel, steps=steps),
            whole,
            col,
            *[outer[k - 1] for k in steps],
            *own,
            spaces="s" + "v" * len(steps) + "hhh",
            outs="hhh",
            scratch=[pltpu.SemaphoreType.DMA((len(steps) * (2 + tp),))],
            alias={len(steps) + 1 + k: k for k in range(3)},
        )
    gate_grad, up_grad, down_grad = own

    inner = ep // lax.axis_size("z")
    group = feat // ep
    hidden_grad, shared = local(
        dots_kernel,
        [half(rows, block), half(inner, ep // inner, group, block)],
        cotangent,
        shared_hidden,
        shared_down,
    )
    shared = over(shared.reshape(feat, block), ("y", "core"))
    shared = local(fold_kernel, half(feat // inner, block), shared)
    shared = over(shared, "z")
    shared_grad = local(total_kernel, jax.ShapeDtypeStruct((feat // ep, block), F32), shared)
    return (
        tokens_grad,
        weights_grad,
        gate_grad.reshape(gate_proj.shape),
        up_grad.reshape(up_proj.shape),
        down_grad.reshape(down_proj.shape),
        hidden_grad,
        shared_grad,
    )


def solution(mesh):
    devices = mesh.devices
    split = Mesh(devices.reshape(8, -1, 2, devices.shape[-1]), (*EP, "tp"))
    return jax.shard_map(
        experts,
        mesh=split,
        in_specs=(
            P(EP, None),
            P(EP, None),
            P(EP, None),
            P(EP, None),
            P(EP, None, "tp"),
            P(EP, None, "tp"),
            P(EP, "tp", None),
            P(None, "tp"),
            P(EP, "tp"),
        ),
        out_specs=(
            P(EP, "tp"),
            P(EP, None),
            P(EP, None, "tp"),
            P(EP, None, "tp"),
            P(EP, "tp", None),
            P(EP, "tp"),
            P(EP, "tp"),
        ),
        check_vma=False,
    )
```
